32 devices in a mesh: rep: 2 (over x), fs: 8 (over z, y), tp: 2 (over core).
Axes of the slice: x: 2, y: 2, z: 4, core: 2. Of those that a mesh axis runs over, the one named last changes fastest.
Arguments:
- x_early: bfloat16 [1792, 2048], P(('rep', 'fs')), may hold values from -6 to 6
- x_late: bfloat16 [1792, 2048], P(('rep', 'fs')), may hold values from -6 to 6
- grad_out: bfloat16 [1792, 2048], P(('rep', 'fs')), may hold values from -6 to 6
- w_gate: bfloat16 [2048, 3072], P('fs', 'tp'), may hold values from -0.125 to 0.125
- w_up: bfloat16 [2048, 3072], P('fs', 'tp'), may hold values from -0.125 to 0.125
- w_down: bfloat16 [3072, 2048], P('tp', 'fs'), may hold values from -0.109375 to 0.109375
- gate_sum: float32 [2048, 3072], P('fs', 'tp'), may hold values from -80 to 80
- up_sum: float32 [2048, 3072], P('fs', 'tp'), may hold values from -80 to 80
- down_sum: float32 [3072, 2048], P('tp', 'fs'), may hold values from -80 to 80
Outputs:
- out_late: bfloat16 [1792, 2048], P(('rep', 'fs'))
- grad_in: bfloat16 [1792, 2048], P(('rep', 'fs'))
- new_gate_sum: float32 [2048, 3072], P('fs', 'tp')
- new_up_sum: float32 [2048, 3072], P('fs', 'tp')
- new_down_sum: float32 [3072, 2048], P('tp', 'fs')
The draws below stay inside these ranges and needn't reach their ends.
All inputs are finite; a program needn't handle non-finite values.
Results may differ from the reference program's by a relative error of at most 0.018.
Values may be sent and summed in bfloat16 or wider, within the bound.
A program may use at most 128 MiB of HBM per device.

```python
import jax
import jax.numpy as jnp
from jax import lax

D = 2048
FF = 3072
TOKENS = 1792
N_TP = 2


def strengthened(drawn, key, source, target, blocks, factor):
    def block_of(dim):
        return (jnp.arange(drawn.shape[dim]) // (drawn.shape[dim] // blocks)).reshape((-1,) + (1,) * (drawn.ndim - 1 - dim))

    one_side = jax.random.permutation(key, blocks)[block_of(target)]
    second = (block_of(target) + blocks // 2) % blocks
    return jnp.where((block_of(source) == one_side) | (block_of(source) == second), factor * drawn, drawn)


def steps_of(rng, extent, split, low, high):
    level, own = 1.0, jax.random.fold_in(rng, 6)
    for position, shards_of in split:
        heights = jnp.exp(jax.random.uniform(jax.random.fold_in(own, position), (shards_of,), jnp.float32, low / len(split), high / len(split)))
        level = level * jnp.repeat(heights, extent[position] // shards_of).reshape([-1 if axis == position else 1 for axis in range(len(extent))])
    return level


def bell_draw(key, extent, scale, most, cuts=(), kind=jnp.bfloat16):
    drawn = jax.random.normal(key, extent, jnp.float32) * scale
    if len(cuts) > 0:
        drawn = steps_of(key, extent, cuts, -0.22, 0.18) * drawn
    return jnp.clip(drawn, min=-most, max=most).astype(kind)


def bell_draw_with(rng, dims, spread, limit, split, heavy, dtype=jnp.bfloat16):
    array = spread * jax.random.normal(rng, dims, jnp.float32)
    if split:
        array = array * steps_of(rng, dims, split, -0.22, 0.18)
    return jnp.clip(strengthened(array, jax.random.fold_in(rng, 3), *heavy), -limit, limit).astype(dtype)


def setup_inputs(seed: int = 0) -> dict:
    seeds = jax.random.split(jax.random.key(seed), 10)
    return {
        "x_early": bell_draw(seeds[0], (TOKENS, D), 1.0, 6.0, ((0, 16),)),
        "x_late": bell_draw(seeds[1], (TOKENS, D), 1.0, 6.0, ((0, 16),)),
        "grad_out": bell_draw_with(seeds[2], (TOKENS, D), 1.0, 6.0, ((0, 16),), (0, 1, 16, 2.0)),
        "w_gate": bell_draw(seeds[3], (D, FF), D ** -0.5, 0.125, ((0, 8), (1, 2))),
        "w_up": bell_draw(seeds[4], (D, FF), D ** -0.5, 0.125, ((0, 8), (1, 2))),
        "w_down": bell_draw(seeds[5], (FF, D), FF ** -0.5, 0.109375, ((0, 2), (1, 8))),
        "gate_sum": bell_draw(seeds[6], (D, FF), (0.3 * TOKENS ** 0.5), 80.0, ((0, 8), (1, 2)), jnp.float32),
        "up_sum": bell_draw(seeds[7], (D, FF), (0.3 * TOKENS ** 0.5), 80.0, ((0, 8), (1, 2)), jnp.float32),
        "down_sum": bell_draw(seeds[8], (FF, D), (0.3 * TOKENS ** 0.5), 80.0, ((0, 2), (1, 8)), jnp.float32),
    }


epsilon = 1e-06

def prepare(x_rows):
    wide = x_rows.astype(jnp.float32)
    row_scale = lax.rsqrt(lax.optimization_barrier(jnp.mean(wide * wide, axis=-1, keepdims=True)) + epsilon)
    normed = (wide * row_scale).astype(jnp.bfloat16)
    return (wide, row_scale, normed)

def reference(x_early, x_late, grad_out, w_gate, w_up, w_down, gate_sum, up_sum, down_sum):
    late_wide, late_scale, late_normed = prepare(x_late)
    late_gate = jnp.dot(late_normed, w_gate, preferred_element_type=jnp.float32)
    late_upper = jnp.dot(late_normed, w_up, preferred_element_type=jnp.float32)
    late_hidden = (late_gate * jax.nn.sigmoid(late_gate) * late_upper).astype(jnp.bfloat16)
    block = FF // N_TP
    branch = jnp.zeros(x_late.shape, jnp.float32)
    for column in range(N_TP):
        part = jnp.dot(late_hidden[:, column * block:(column + 1) * block], w_down[column * block:(column + 1) * block], preferred_element_type=jnp.float32)
        branch = branch + part.astype(jnp.bfloat16).astype(jnp.float32)
    out_late = (late_wide + 0.5 * branch).astype(jnp.bfloat16)
    early_wide, early_scale, early_normed = prepare(x_early)
    gate_pre = jnp.dot(early_normed, w_gate, preferred_element_type=jnp.float32)
    up_pre = jnp.dot(early_normed, w_up, preferred_element_type=jnp.float32)
    gate_sig = jax.nn.sigmoid(gate_pre)
    hidden = (gate_pre * gate_sig * up_pre).astype(jnp.bfloat16)
    grad_hidden = 0.5 * jnp.dot(grad_out, w_down.T, preferred_element_type=jnp.float32)
    grad_gate_in = (grad_hidden * up_pre * gate_sig * (1.0 + gate_pre * (1.0 - gate_sig))).astype(jnp.bfloat16)
    grad_up_in = (grad_hidden * gate_pre * gate_sig).astype(jnp.bfloat16)
    grad_normed = jnp.dot(grad_gate_in, w_gate.T, preferred_element_type=jnp.float32)
    grad_normed = grad_normed + jnp.dot(grad_up_in, w_up.T, preferred_element_type=jnp.float32)
    unit_rows = early_wide * early_scale
    inner = lax.optimization_barrier(jnp.mean(grad_normed * unit_rows, axis=-1, keepdims=True))
    grad_in = (grad_out.astype(jnp.float32) + early_scale * (grad_normed - unit_rows * inner)).astype(jnp.bfloat16)
    new_gate_sum = gate_sum + jnp.dot(early_normed.T, grad_gate_in, preferred_element_type=jnp.float32)
    new_up_sum = up_sum + jnp.dot(early_normed.T, grad_up_in, preferred_element_type=jnp.float32)
    new_down_sum = down_sum + 0.5 * jnp.dot(hidden.T, grad_out, preferred_element_type=jnp.float32)
    return (out_late, grad_in, new_gate_sum, new_up_sum, new_down_sum)
```

```python
import functools

import jax
import jax.numpy as jnp
from jax import lax
from jax.experimental import pallas as pl
from jax.experimental.pallas import tpu as pltpu
from jax.sharding import PartitionSpec as P

epsilon = 1e-06
MESH = pl.DeviceIdType.MESH
ANY = pl.BlockSpec(memory_space=pl.ANY)
LANES, ROWS = 128, 16


def contract_rows(left, right):
    return lax.dot_general(
        left, right, (((0,), (0,)), ((), ())), preferred_element_type=jnp.float32
    )


def contract_cols(left, right):
    return lax.dot_general(
        left, right, (((1,), (1,)), ((), ())), preferred_element_type=jnp.float32
    )


def greet(peers):
    barrier = pltpu.get_barrier_semaphore()
    for peer in peers:
        pl.semaphore_signal(barrier, inc=1, device_id=peer, device_id_type=MESH)
    pl.semaphore_wait(barrier, len(peers))


def push(src, dst, send_sem, recv_sem, peer):
    copy = pltpu.make_async_remote_copy(
        src_ref=src,
        dst_ref=dst,
        send_sem=send_sem,
        recv_sem=recv_sem,
        device_id=peer,
        device_id_type=MESH,
    )
    return copy


def block(index, size, unit):
    return pl.ds(pl.multiple_of(index * size, unit), size)


def add_strips(dst, left, right):
    @pl.loop(0, dst.shape[0] // ROWS)
    def _(i):
        at = block(i, ROWS, ROWS)
        total = left[at, :].astype(jnp.float32) + right[at, :].astype(jnp.float32)
        dst[at, :] = total.astype(dst.dtype)


def scale_of(v):
    return lax.rsqrt(jnp.mean(v * v, axis=-1, keepdims=True) + epsilon)


def step_kernel(
    n,
    x_early,
    x_late,
    grad_out,
    w_gate,
    w_up,
    w_down,
    out_late,
    grad_in,
    delta_gate,
    delta_up,
    delta_down,
    acts,
    gate_up,
    down,
    hidden,
    grads,
    part,
    part_in,
    sums,
    from_below,
    from_above,
    gate_up_delta,
    down_delta,
    y_gate_up,
    y_down,
    x_gate_up,
    x_down,
    full,
    send,
    recv,
    local,
):
    f32, bf16 = jnp.float32, jnp.bfloat16
    rep, fs, tp = lax.axis_index("rep"), lax.axis_index("fs"), lax.axis_index("tp")
    line = n // 2
    z, y = fs // 2, lax.rem(fs, 2)
    twin, mate, side = {"rep": 1 - rep}, {"tp": 1 - tp}, {"fs": fs + 1 - 2 * y}
    above, below = {"fs": lax.rem(fs + 2, n)}, {"fs": lax.rem(fs + n - 2, n)}
    rows, width = x_early.shape
    layer, depth = down.shape[0], w_gate.shape[0]
    half, deep, tall = width // 2, depth // 2, layer // 2
    mine, other = block(tp, half, LANES), block(1 - tp, half, LANES)
    names, pending = {}, []
    last = line - 1

    def at(*key):
        return names.setdefault(key, len(names))

    def copies(key, srcs, dsts, peer):
        return [
            push(s, d, send.at[at(key, i)], recv.at[at(key, i)], peer)
            for i, (s, d) in enumerate(zip(srcs, dsts))
        ]

    def go(group, cond=None):
        def start():
            for copy in group:
                copy.start()

        pending.append((cond, group))
        if cond is None:
            start()
        else:
            pl.when(cond)(start)

    def arrived(key, refs):
        for copy in copies(key, refs, refs, twin):
            copy.wait_recv()

    def place(k):
        return lax.rem(z + k, line)

    def origin(k):
        return lax.rem(z + line - k, line)

    def slice3(owner, who):
        at_rows = block(owner * 2 + who, deep, ROWS)
        return [
            gate_up.at[at_rows, pl.ds(0, layer)],
            gate_up.at[at_rows, pl.ds(layer, layer)],
            down.at[block(who, tall, ROWS), block(owner, depth, LANES)],
        ]

    def slice2(owner, who):
        return [
            gate_up.at[block(owner * 2 + who, deep, ROWS), :],
            down.at[block(who, tall, ROWS), block(owner, depth, LANES)],
        ]

    def whole3(owner):
        at_rows = block(owner, depth, ROWS)
        return [
            gate_up.at[at_rows, pl.ds(0, layer)],
            gate_up.at[at_rows, pl.ds(layer, layer)],
            down.at[:, block(owner, depth, LANES)],
        ]

    def source3(to):
        at_rows, at_cols = block(rep, deep, ROWS), block(to, layer, LANES)
        return [
            w_gate.at[at_rows, at_cols],
            w_up.at[at_rows, at_cols],
            w_down.at[block(to * 2 + rep, tall, ROWS), :],
        ]

    own_source = [
        w_gate.at[:, block(z, layer, LANES)],
        w_up.at[:, block(z, layer, LANES)],
        w_down.at[block(z, layer, ROWS), :],
    ]
    own_rows = block(z, rows, ROWS)
    keeps = [
        pltpu.make_async_copy(s, d, local.at[i])
        for i, (s, d) in enumerate(zip(own_source, whole3(fs)))
    ]
    keeps.append(pltpu.make_async_copy(grad_out, acts.at[1, own_rows, :], local.at[3]))
    for keep in keeps:
        keep.start()

    barrier = pltpu.get_barrier_semaphore()
    peers = [twin, mate, side] + [{"fs": lax.rem(fs + 2 * k, n)} for k in range(1, line)]
    for peer in peers:
        pl.semaphore_signal(barrier, inc=1, device_id=peer, device_id_type=MESH)
    pl.semaphore_wait(barrier, len(peers))

    for k in sorted(range(1, line), key=lambda k: -min(k, line - k)):
        to = {"fs": lax.rem(fs + 2 * k, n)}
        go(copies(("wz", k), source3(place(k)), slice3(fs, rep), to))
    go(copies("wy0", own_source, whole3(fs), side))

    def normalise(i, x):
        @pl.loop(0, rows // ROWS)
        def _(j):
            v = x[block(j, ROWS, ROWS), :].astype(f32)
            to = pl.ds(pl.multiple_of(z * rows + j * ROWS, ROWS), ROWS)
            acts[i, to, :] = (v * scale_of(v)).astype(bf16)

    def spot(i, place_of, cols=mine):
        return acts.at[i, block(place_of, rows, ROWS), cols]

    def go_up(i, s):
        src = grad_out.at[:, mine] if i == 1 and s == 0 else spot(i, z - s)
        go(copies(("up", i, s), [src], [spot(i, z - s)], above), (z - s >= 0) & (z < last))

    def go_down(i, s):
        src = grad_out.at[:, mine] if i == 1 and s == 0 else spot(i, z + s)
        go(copies(("down", i, s), [src], [spot(i, z + s)], below), (z + s < line) & (z > 0))

    def move(i, s):
        under, over = z - 1 - s, z + 1 + s
        pl.when(under >= 0)(lambda: arrived(("up", i, s), [spot(i, under)]))
        if s + 1 < last:
            go_up(i, s + 1)
        go(copies(("mu", i, s), [spot(i, under)], [spot(i, under)], mate), under >= 0)
        pl.when(over < line)(lambda: arrived(("down", i, s), [spot(i, over)]))
        if s + 1 < last:
            go_down(i, s + 1)
        go(copies(("md", i, s), [spot(i, over)], [spot(i, over)], mate), over < line)

    def moved(i, s):
        under, over = z - 1 - s, z + 1 + s
        pl.when(under >= 0)(lambda: arrived(("mu", i, s), [spot(i, under, other)]))
        pl.when(over < line)(lambda: arrived(("md", i, s), [spot(i, over, other)]))

    def first(i):
        go_up(i, 0)
        go_down(i, 0)

    first(1)
    normalise(0, x_early)
    first(0)
    normalise(2, x_late)

    for k in range(1, line):
        part2 = slice2(origin(k) * 2 + y, rep)
        arrived(("wz", k), slice3(origin(k) * 2 + y, rep))
        go(copies(("wy", k), part2, part2, side))
        go(copies(("wx", k), part2, part2, twin))

    def pass_on(k):
        part2 = slice2(origin(k) * 2 + 1 - y, rep)
        arrived(("wy", k), part2)
        go(copies(("wxx", k), part2, part2, twin))

    for s in range(last - 1):
        move(1, s)
        move(0, s)
        pass_on(s + 1)
    first(2)
    for k in range(max(last, 1), line):
        pass_on(k)
    for keep in keeps:
        keep.wait()
    arrived("wy0", whole3(fs + 1 - 2 * y))
    for k in range(1, line):
        arrived(("wx", k), slice2(origin(k) * 2 + y, 1 - rep))
        arrived(("wxx", k), slice2(origin(k) * 2 + 1 - y, 1 - rep))

    def activations(x):
        pre = jnp.dot(x, gate_up[...], preferred_element_type=f32)
        g, u = pre[:, :layer], pre[:, layer:]
        s = jax.nn.sigmoid(g)
        return g, u, s, (g * s * u).astype(bf16)

    def early_block(place_of):
        here = block(place_of, rows, ROWS)
        g, u, s, h = activations(acts[0, here, :])
        grad_hidden = 0.5 * contract_cols(acts[1, here, :], down[...])
        hidden[here, :] = h
        grads[here, pl.ds(0, layer)] = (grad_hidden * u * s * (1.0 + g * (1.0 - s))).astype(bf16)
        grads[here, pl.ds(layer, layer)] = (grad_hidden * g * s).astype(bf16)

    early_block(z)
    for s in range(last):
        if s == last - 1:
            move(1, s)
            move(0, s)
        moved(1, s)
        moved(0, s)

        @pl.loop(0, 2)
        def _(d):
            to = z + (2 * d - 1) * (s + 1)
            pl.when((to >= 0) & (to < line))(lambda: early_block(to))

    order = list(range(1, line)) + [0]

    def weight_grads(owner):
        cols = block(owner, depth, LANES)
        gate_up_delta[block(owner, depth, ROWS), :] = contract_rows(
            acts[0, :, cols], grads[...]
        ).astype(bf16)
        down_delta[:, cols] = (0.5 * contract_rows(hidden[...], acts[1, :, cols])).astype(bf16)

    def deltas(owner):
        return [
            gate_up_delta.at[block(owner, depth, ROWS), :],
            down_delta.at[:, block(owner, depth, LANES)],
        ]

    for k in order:
        owner = place(k) * 2 + 1 - y
        weight_grads(owner)
        go(copies(("gy", k), deltas(owner), [y_gate_up.at[place(k)], y_down.at[place(k)]], side))

    @pl.loop(0, line)
    def _(t):
        weight_grads(t * 2 + y)

    wide = next(b for b in (512, 256, 128) if width % b == 0)

    @pl.loop(0, width // wide)
    def _(j):
        cols = block(j, wide, LANES)
        part[1, :, cols] = contract_cols(grads[...], gate_up[block(j, wide, ROWS), :]).astype(bf16)

    def to_mate(i):
        go(copies(("pm", i), [part.at[i, :, other]], [part_in.at[i]], mate))

    def from_mate(i):
        arrived(("pm", i), [part_in.at[i]])

        @pl.loop(0, line)
        def _(t):
            here = block(t, rows, ROWS)
            add_strips(sums.at[i, t], part.at[i, here, mine], part_in.at[i, here, :])

    def chain(i):
        for d in range(last):
            t = last - d

            def add_up():
                arrived(("zu", i, t), [from_below.at[i, t]])
                add_strips(sums.at[i, t], sums.at[i, t], from_below.at[i, t])

            pl.when((z >= 1) & (z < t))(add_up)
            go(copies(("zu", i, t), [sums.at[i, t]], [from_below.at[i, t]], above), z < t)

            def add_down():
                arrived(("zd", i, d), [from_above.at[i, d]])
                add_strips(sums.at[i, d], sums.at[i, d], from_above.at[i, d])

            pl.when((z < last) & (z > d))(add_down)
            go(copies(("zd", i, d), [sums.at[i, d]], [from_above.at[i, d]], below), z > d)

    def finish(i):
        for t in range(line):
            if t > 0:

                def add_up():
                    arrived(("zu", i, t), [from_below.at[i, t]])
                    add_strips(sums.at[i, t], sums.at[i, t], from_below.at[i, t])

                pl.when(z == t)(add_up)
            if t < last:

                def add_down():
                    arrived(("zd", i, t), [from_above.at[i, t]])
                    add_strips(sums.at[i, t], sums.at[i, t], from_above.at[i, t])

                pl.when(z == t)(add_down)
        full[i, :, mine] = sums[i, z]
        go(copies(("fm", i), [full.at[i, :, mine]], [full.at[i, :, mine]], mate))

    def outputs():
        for i in range(2):
            arrived(("fm", i), [full.at[i, :, other]])

        @pl.loop(0, rows // ROWS)
        def _(j):
            here = block(j, ROWS, ROWS)
            late = x_late[here, :].astype(f32)
            out_late[here, :] = (late + 0.5 * full[0, here, :].astype(f32)).astype(bf16)
            early = x_early[here, :].astype(f32)
            scale = scale_of(early)
            unit = early * scale
            grad_normed = full[1, here, :].astype(f32)
            inner = jnp.mean(grad_normed * unit, axis=-1, keepdims=True)
            kept = acts[1, pl.ds(pl.multiple_of(z * rows + j * ROWS, ROWS), ROWS), :].astype(f32)
            grad_in[here, :] = (kept + scale * (grad_normed - unit * inner)).astype(bf16)

    def y_step(k):
        t = place(k)
        arrived(("gy", k), [y_gate_up.at[t], y_down.at[t]])
        own = deltas(t * 2 + y)
        add_strips(y_gate_up.at[t], own[0], y_gate_up.at[t])
        add_strips(y_down.at[t], own[1], y_down.at[t])
        srcs = [
            y_gate_up.at[t, block(1 - rep, deep, ROWS), :],
            y_down.at[t, block(1 - rep, tall, ROWS), :],
        ]
        go(copies(("gx", k), srcs, [x_gate_up.at[t], x_down.at[t]], twin))

    def landing(place_of, who):
        at_rows, at_cols = block(who, deep, ROWS), block(place_of, layer, LANES)
        return [
            delta_gate.at[at_rows, at_cols],
            delta_up.at[at_rows, at_cols],
            delta_down.at[block(place_of * 2 + who, tall, ROWS), :],
        ]

    puts = []

    def x_step(k):
        t = place(k)
        arrived(("gx", k), [x_gate_up.at[t], x_down.at[t]])
        add_strips(x_gate_up.at[t], y_gate_up.at[t, block(rep, deep, ROWS), :], x_gate_up.at[t])
        add_strips(x_down.at[t], y_down.at[t, block(rep, tall, ROWS), :], x_down.at[t])
        srcs = [
            x_gate_up.at[t, :, pl.ds(0, layer)],
            x_gate_up.at[t, :, pl.ds(layer, layer)],
            x_down.at[t],
        ]
        if k:
            go(copies(("gz", k), srcs, landing(z, rep), {"fs": lax.rem(fs + 2 * k, n)}))
            return
        go(copies(("gt", 0), srcs, landing(z, rep), twin))
        for i, (s, d) in enumerate(zip(srcs, landing(z, rep))):
            put = pltpu.make_async_copy(s, d, local.at[i])
            put.start()
            puts.append(put)

    def z_step(k):
        refs = landing(origin(k), rep)
        arrived(("gz", k), refs)
        go(copies(("gt", k), refs, refs, twin))

    to_mate(1)
    for s in range(last):
        move(2, s)
    from_mate(1)
    chain(1)
    for s in range(last):
        moved(2, s)

    @pl.loop(0, line)
    def _(t):
        here = block(t, rows, ROWS)
        hidden[here, :] = activations(acts[2, here, :])[3]

    @pl.loop(0, width // wide)
    def _(j):
        cols = block(j, wide, LANES)
        part[0, :, cols] = jnp.dot(
            hidden[...], down[:, cols], preferred_element_type=f32
        ).astype(bf16)

    to_mate(0)
    y_step(order[0])
    from_mate(0)
    chain(0)
    x_step(order[0])
    finish(1)
    y_step(order[1])
    finish(0)
    z_step(order[0])
    x_step(order[1])
    for i in range(2, line):
        y_step(order[i])
        z_step(order[i - 1])
        if i == line - 1:
            outputs()
        x_step(order[i])
    if line == 2:
        outputs()
    for k in order:
        arrived(("gt", k), landing(origin(k), 1 - rep))
    for put in puts:
        put.wait()
    assert len(names) <= send.shape[0]
    for cond, group in pending:

        def drain():
            for copy in group:
                copy.wait_send()

        if cond is None:
            drain()
        else:
            pl.when(cond)(drain)


def fast_shards(n, x_early, x_late, grad_out, w_gate, w_up, w_down, gate_sum, up_sum, down_sum):
    bf16 = jnp.bfloat16
    shape = jax.ShapeDtypeStruct
    line = n // 2
    rows, width = x_early.shape
    hidden_here, depth = w_down.shape
    layer = hidden_here // line
    tokens, half = line * rows, width // 2
    dma, vmem = pltpu.SemaphoreType.DMA, pl.BlockSpec(memory_space=pltpu.VMEM)
    count = 50 * line
    out_late, grad_in, delta_gate, delta_up, delta_down = pl.pallas_call(
        functools.partial(step_kernel, n),
        out_shape=[
            shape((rows, width), bf16),
            shape((rows, width), bf16),
            shape((depth, hidden_here), bf16),
            shape((depth, hidden_here), bf16),
            shape((hidden_here, depth), bf16),
        ],
        in_specs=[vmem, vmem, ANY, ANY, ANY, ANY],
        out_specs=[vmem, vmem, ANY, ANY, ANY],
        scratch_shapes=[
            pltpu.VMEM((3, tokens, width), bf16),
            pltpu.VMEM((width, 2 * layer), bf16),
            pltpu.VMEM((layer, width), bf16),
            pltpu.VMEM((tokens, layer), bf16),
            pltpu.VMEM((tokens, 2 * layer), bf16),
            pltpu.VMEM((2, tokens, width), bf16),
            pltpu.VMEM((2, tokens, half), bf16),
            pltpu.VMEM((2, line, rows, half), bf16),
            pltpu.VMEM((2, line, rows, half), bf16),
            pltpu.VMEM((2, line, rows, half), bf16),
            pltpu.VMEM((width, 2 * layer), bf16),
            pltpu.VMEM((layer, width), bf16),
            pltpu.VMEM((line, depth, 2 * layer), bf16),
            pltpu.VMEM((line, layer, depth), bf16),
            pltpu.VMEM((line, depth // 2, 2 * layer), bf16),
            pltpu.VMEM((line, layer // 2, depth), bf16),
            pltpu.VMEM((2, rows, width), bf16),
            dma((count,)),
            dma((count,)),
            dma((4,)),
        ],
        compiler_params=pltpu.CompilerParams(
            collective_id=0, has_side_effects=True, vmem_limit_bytes=56 * 2**20
        ),
    )(x_early, x_late, grad_out, w_gate, w_up, w_down)
    return (
        out_late,
        grad_in,
        gate_sum + delta_gate.astype(jnp.float32),
        up_sum + delta_up.astype(jnp.float32),
        down_sum + delta_down.astype(jnp.float32),
    )


def shards(x_early, x_late, grad_out, w_gate, w_up, w_down, gate_sum, up_sum, down_sum):
    gate_full, up_full, down_full = (
        lax.all_gather(w_gate, "fs", axis=0, tiled=True),
        lax.all_gather(w_up, "fs", axis=0, tiled=True),
        lax.all_gather(w_down, "fs", axis=1, tiled=True),
    )
    batch_rows = x_early.shape[0]
    stacked = jnp.concatenate([x_early, x_late], axis=0).astype(jnp.float32)
    row_scale = lax.rsqrt(jnp.mean(stacked * stacked, axis=-1, keepdims=True) + epsilon)
    normed = (stacked * row_scale).astype(jnp.bfloat16)
    gate_pre = jnp.dot(normed, gate_full, preferred_element_type=jnp.float32)
    up_pre = jnp.dot(normed, up_full, preferred_element_type=jnp.float32)
    gate_sig = jax.nn.sigmoid(gate_pre)
    hidden = (gate_pre * gate_sig * up_pre).astype(jnp.bfloat16)
    late_part = jnp.dot(hidden[batch_rows:], down_full, preferred_element_type=jnp.float32).astype(
        jnp.bfloat16
    )
    branch = lax.psum(late_part, "tp").astype(jnp.float32)
    out_late = (stacked[batch_rows:] + 0.5 * branch).astype(jnp.bfloat16)
    early_gate = gate_pre[:batch_rows]
    early_upper = up_pre[:batch_rows]
    early_sig = gate_sig[:batch_rows]
    early_hidden = hidden[:batch_rows]
    early_normed = normed[:batch_rows]
    early_scale = row_scale[:batch_rows]
    grad_hidden = 0.5 * contract_cols(grad_out, down_full)
    grad_gate_in = (
        grad_hidden * early_upper * early_sig * (1.0 + early_gate * (1.0 - early_sig))
    ).astype(jnp.bfloat16)
    grad_up_in = (grad_hidden * early_gate * early_sig).astype(jnp.bfloat16)
    normed_part = contract_cols(grad_gate_in, gate_full) + contract_cols(grad_up_in, up_full)
    grad_normed = lax.psum(normed_part.astype(jnp.bfloat16), "tp").astype(jnp.float32)
    unit_rows = stacked[:batch_rows] * early_scale
    inner = jnp.mean(grad_normed * unit_rows, axis=-1, keepdims=True)
    grad_in = (
        grad_out.astype(jnp.float32) + early_scale * (grad_normed - unit_rows * inner)
    ).astype(jnp.bfloat16)
    normed_cols, out_cols = (
        lax.all_to_all(early_normed, "fs", split_axis=1, concat_axis=0, tiled=True),
        lax.all_to_all(grad_out, "fs", split_axis=1, concat_axis=0, tiled=True),
    )
    gate_delta = contract_rows(normed_cols, lax.all_gather(grad_gate_in, "fs", axis=0, tiled=True))
    up_delta = contract_rows(normed_cols, lax.all_gather(grad_up_in, "fs", axis=0, tiled=True))
    down_half = contract_rows(lax.all_gather(early_hidden, "fs", axis=0, tiled=True), out_cols)
    down_delta = 0.5 * down_half
    gate_delta, up_delta, down_delta = (
        lax.psum(gate_delta.astype(jnp.bfloat16), "rep").astype(jnp.float32),
        lax.psum(up_delta.astype(jnp.bfloat16), "rep").astype(jnp.float32),
        lax.psum(down_delta.astype(jnp.bfloat16), "rep").astype(jnp.float32),
    )
    return (out_late, grad_in, gate_sum + gate_delta, up_sum + up_delta, down_sum + down_delta)


def shards_for(mesh):
    n, reps, cores = mesh.shape["fs"], mesh.shape["rep"], mesh.shape["tp"]

    def run(*args):
        rows, width = args[0].shape
        hidden_here, depth = args[5].shape
        line = max(n // 2, 1)
        layer = hidden_here // line
        fits = (
            reps == 2
            and cores == 2
            and n % 2 == 0
            and n >= 4
            and rows % ROWS == 0
            and width % (2 * LANES) == 0
            and depth % (2 * LANES) == 0
            and hidden_here % line == 0
            and layer % LANES == 0
            and layer % (2 * ROWS) == 0
            and 2 * (10 * line * rows * width + 10 * width * layer) < 44 * 2**20
        )
        return fast_shards(n, *args) if fits else shards(*args)

    return run


def solution(mesh):
    placed = (
        P(("rep", "fs"), None),
        P(("rep", "fs"), None),
        P(("rep", "fs"), None),
        P("fs", "tp"),
        P("fs", "tp"),
        P("tp", "fs"),
        P("fs", "tp"),
        P("fs", "tp"),
        P("tp", "fs"),
    )
    return jax.shard_map(
        shards_for(mesh),
        mesh=mesh,
        in_specs=placed,
        out_specs=(
            P(("rep", "fs"), None),
            P(("rep", "fs"), None),
            P("fs", "tp"),
            P("fs", "tp"),
            P("tp", "fs"),
        ),
        check_vma=False,
    )
```

```python
import functools

import jax
import jax.numpy as jnp
from jax import lax
from jax.experimental import pallas as pl
from jax.experimental.pallas import tpu as pltpu
from jax.sharding import PartitionSpec as P

epsilon = 1e-06
MESH = pl.DeviceIdType.MESH
ANY = pl.BlockSpec(memory_space=pl.ANY)
LANES, ROWS = 128, 16


def contract_rows(left, right):
    return lax.dot_general(
        left, right, (((0,), (0,)), ((), ())), preferred_element_type=jnp.float32
    )


def contract_cols(left, right):
    return lax.dot_general(
        left, right, (((1,), (1,)), ((), ())), preferred_element_type=jnp.float32
    )


def greet(peers):
    barrier = pltpu.get_barrier_semaphore()
    for peer in peers:
        pl.semaphore_signal(barrier, inc=1, device_id=peer, device_id_type=MESH)
    pl.semaphore_wait(barrier, len(peers))


def push(src, dst, send_sem, recv_sem, peer):
    copy = pltpu.make_async_remote_copy(
        src_ref=src,
        dst_ref=dst,
        send_sem=send_sem,
        recv_sem=recv_sem,
        device_id=peer,
        device_id_type=MESH,
    )
    return copy


def block(index, size, unit):
    return pl.ds(pl.multiple_of(index * size, unit), size)


def add_strips(dst, left, right):
    @pl.loop(0, dst.shape[0] // ROWS)
    def _(i):
        at = block(i, ROWS, ROWS)
        total = left[at, :].astype(jnp.float32) + right[at, :].astype(jnp.float32)
        dst[at, :] = total.astype(dst.dtype)


def named(f):
    def g(*args):
        tags = [str(a) for a in args if isinstance(a, int)]
        with jax.named_scope("_".join([f.__name__.strip("_")] + tags)):
            return f(*args)

    return g


def scale_of(v):
    return lax.rsqrt(jnp.mean(v * v, axis=-1, keepdims=True) + epsilon)


def step_kernel(
    n,
    x_early,
    x_late,
    grad_out,
    w_gate,
    w_up,
    w_down,
    out_late,
    grad_in,
    delta_gate,
    delta_up,
    delta_down,
    acts,
    gate_up,
    down,
    hidden,
    grads,
    part,
    part_in,
    sums,
    from_below,
    from_above,
    gate_up_delta,
    down_delta,
    y_gate_up,
    y_down,
    x_gate_up,
    x_down,
    full,
    send,
    recv,
    local,
):
    f32, bf16 = jnp.float32, jnp.bfloat16
    rep, fs, tp = lax.axis_index("rep"), lax.axis_index("fs"), lax.axis_index("tp")
    line = n // 2
    z, y = fs // 2, lax.rem(fs, 2)
    twin, mate, side = {"rep": 1 - rep}, {"tp": 1 - tp}, {"fs": fs + 1 - 2 * y}
    above, below = {"fs": lax.rem(fs + 2, n)}, {"fs": lax.rem(fs + n - 2, n)}
    rows, width = x_early.shape
    layer, depth = down.shape[0], w_gate.shape[0]
    half, deep, tall = width // 2, depth // 2, layer // 2
    mine, other = block(tp, half, LANES), block(1 - tp, half, LANES)
    names, pending = {}, []
    last = line - 1

    def at(*key):
        return names.setdefault(key, len(names))

    def copies(key, srcs, dsts, peer):
        return [
            push(s, d, send.at[at(key, i)], recv.at[at(key, i)], peer)
            for i, (s, d) in enumerate(zip(srcs, dsts))
        ]

    def go(group, cond=None):
        def start():
            for copy in group:
                copy.start()

        pending.append((cond, group))
        if cond is None:
            start()
        else:
            pl.when(cond)(start)

    def arrived(key, refs):
        for copy in copies(key, refs, refs, twin):
            copy.wait_recv()

    def place(k):
        return lax.rem(z + k, line)

    def origin(k):
        return lax.rem(z + line - k, line)

    def slice3(owner, who):
        at_rows = block(owner * 2 + who, deep, ROWS)
        return [
            gate_up.at[at_rows, pl.ds(0, layer)],
            gate_up.at[at_rows, pl.ds(layer, layer)],
            down.at[block(who, tall, ROWS), block(owner, depth, LANES)],
        ]

    def slice2(owner, who):
        return [
            gate_up.at[block(owner * 2 + who, deep, ROWS), :],
            down.at[block(who, tall, ROWS), block(owner, depth, LANES)],
        ]

    def whole3(owner):
        at_rows = block(owner, depth, ROWS)
        return [
            gate_up.at[at_rows, pl.ds(0, layer)],
            gate_up.at[at_rows, pl.ds(layer, layer)],
            down.at[:, block(owner, depth, LANES)],
        ]

    def source3(to):
        at_rows, at_cols = block(rep, deep, ROWS), block(to, layer, LANES)
        return [
            w_gate.at[at_rows, at_cols],
            w_up.at[at_rows, at_cols],
            w_down.at[block(to * 2 + rep, tall, ROWS), :],
        ]

    own_source = [
        w_gate.at[:, block(z, layer, LANES)],
        w_up.at[:, block(z, layer, LANES)],
        w_down.at[block(z, layer, ROWS), :],
    ]
    own_rows = block(z, rows, ROWS)
    keeps = [
        pltpu.make_async_copy(s, d, local.at[i])
        for i, (s, d) in enumerate(zip(own_source, whole3(fs)))
    ]
    keeps.append(pltpu.make_async_copy(grad_out, acts.at[1, own_rows, :], local.at[3]))
    for keep in keeps:
        keep.start()

    barrier = pltpu.get_barrier_semaphore()
    enter = jax.named_scope("enter")
    enter.__enter__()
    peers = [twin, mate, side] + [{"fs": lax.rem(fs + 2 * k, n)} for k in range(1, line)]
    for peer in peers:
        pl.semaphore_signal(barrier, inc=1, device_id=peer, device_id_type=MESH)
    pl.semaphore_wait(barrier, len(peers))
    enter.__exit__(None, None, None)

    for d in [1] + list(range(last, 1, -1)):
        up, low = {"fs": lax.rem(fs + 2 * d, n)}, {"fs": lax.rem(fs + n - 2 * d, n)}
        go(copies(("wu", d), source3(z + d), slice3(fs, rep), up), z + d < line)
        go(copies(("wd", d), source3(z - d), slice3(fs, rep), low), z - d >= 0)
    go(copies("wy0", own_source, whole3(fs), side))

    @named
    def normalise(i, x):
        @pl.loop(0, rows // ROWS)
        def _(j):
            v = x[block(j, ROWS, ROWS), :].astype(f32)
            to = pl.ds(pl.multiple_of(z * rows + j * ROWS, ROWS), ROWS)
            acts[i, to, :] = (v * scale_of(v)).astype(bf16)

    def spot(i, place_of, cols=mine):
        return acts.at[i, block(place_of, rows, ROWS), cols]

    def go_up(i, s):
        src = grad_out.at[:, mine] if i == 1 and s == 0 else spot(i, z - s)
        go(copies(("up", i, s), [src], [spot(i, z - s)], above), (z - s >= 0) & (z < last))

    def go_down(i, s):
        src = grad_out.at[:, mine] if i == 1 and s == 0 else spot(i, z + s)
        go(copies(("down", i, s), [src], [spot(i, z + s)], below), (z + s < line) & (z > 0))

    @named
    def move(i, s):
        under, over = z - 1 - s, z + 1 + s
        pl.when(under >= 0)(lambda: arrived(("up", i, s), [spot(i, under)]))
        if s + 1 < last:
            go_up(i, s + 1)
        go(copies(("mu", i, s), [spot(i, under)], [spot(i, under)], mate), under >= 0)
        pl.when(over < line)(lambda: arrived(("down", i, s), [spot(i, over)]))
        if s + 1 < last:
            go_down(i, s + 1)
        go(copies(("md", i, s), [spot(i, over)], [spot(i, over)], mate), over < line)

    @named
    def moved(i, s):
        under, over = z - 1 - s, z + 1 + s
        pl.when(under >= 0)(lambda: arrived(("mu", i, s), [spot(i, under, other)]))
        pl.when(over < line)(lambda: arrived(("md", i, s), [spot(i, over, other)]))

    def first(i):
        go_up(i, 0)
        go_down(i, 0)

    first(1)
    normalise(0, x_early)
    first(0)
    normalise(2, x_late)

    def layers(d):
        return (("wu", z - d, z - d >= 0), ("wd", z + d, z + d < line))

    def on(cond, f):
        pl.when(cond)(f)

    @named
    def weights_in(d):
        for tag, at_z, cond in layers(d):
            part2 = slice2(at_z * 2 + y, rep)
            on(cond, lambda: arrived((tag, d), slice3(at_z * 2 + y, rep)))
            go(copies((tag, "y", d), part2, part2, side), cond)
            go(copies((tag, "x", d), part2, part2, twin), cond)

    def turned(d):
        return d == 2

    @named
    def relay(d):
        for tag, at_z, cond in layers(d):
            if turned(d):
                part2, key, peer = slice2(at_z * 2 + y, 1 - rep), "x", side
            else:
                part2, key, peer = slice2(at_z * 2 + 1 - y, rep), "y", twin
            on(cond, lambda: arrived((tag, key, d), part2))
            go(copies((tag, "xy", d), part2, part2, peer), cond)

    @named
    def weights_done(d):
        for tag, at_z, cond in layers(d):
            if turned(d):
                part2, key = slice2(at_z * 2 + 1 - y, rep), "y"
            else:
                part2, key = slice2(at_z * 2 + y, 1 - rep), "x"
            on(cond, lambda: arrived((tag, key, d), part2))
            on(cond, lambda: arrived((tag, "xy", d), slice2(at_z * 2 + 1 - y, 1 - rep)))

    weights_in(1)
    if line > 2:
        weights_in(last)
    for s in range(last - 1):
        relay(s + 1 if s == 0 else last + 1 - s)
        move(1, s)
        if last - 1 - s > 1:
            weights_in(last - 1 - s)
        move(0, s)
    first(2)
    if line > 2:
        relay(2)
    else:
        relay(1)
    with jax.named_scope("weights_wait"):
        for keep in keeps:
            keep.wait()
        arrived("wy0", whole3(fs + 1 - 2 * y))
    for d in range(1, line):
        weights_done(d)

    def activations(x):
        pre = jnp.dot(x, gate_up[...], preferred_element_type=f32)
        g, u = pre[:, :layer], pre[:, layer:]
        s = jax.nn.sigmoid(g)
        return g, u, s, (g * s * u).astype(bf16)

    def early_block(place_of):
        here = block(place_of, rows, ROWS)
        g, u, s, h = activations(acts[0, here, :])
        grad_hidden = 0.5 * contract_cols(acts[1, here, :], down[...])
        hidden[here, :] = h
        grads[here, pl.ds(0, layer)] = (grad_hidden * u * s * (1.0 + g * (1.0 - s))).astype(bf16)
        grads[here, pl.ds(layer, layer)] = (grad_hidden * g * s).astype(bf16)

    with jax.named_scope("early_own"):
        early_block(z)
    for s in range(last):
        if s == last - 1:
            for earlier in range(last - 2):
                move(2, earlier)
            move(1, s)
            move(0, s)
        moved(1, s)
        moved(0, s)

        with jax.named_scope(f"early_{s}"):

            @pl.loop(0, 2)
            def _(d):
                to = z + (2 * d - 1) * (s + 1)
                pl.when((to >= 0) & (to < line))(lambda: early_block(to))

    order = list(range(1, line)) + [0]

    def weight_grads(owner):
        cols = block(owner, depth, LANES)
        gate_up_delta[block(owner, depth, ROWS), :] = contract_rows(
            acts[0, :, cols], grads[...]
        ).astype(bf16)
        down_delta[:, cols] = (0.5 * contract_rows(hidden[...], acts[1, :, cols])).astype(bf16)

    def deltas(owner):
        return [
            gate_up_delta.at[block(owner, depth, ROWS), :],
            down_delta.at[:, block(owner, depth, LANES)],
        ]

    for k in order:
        owner = place(k) * 2 + 1 - y
        with jax.named_scope(f"wgrad_{k}"):
            weight_grads(owner)
        ref_gate_up, ref_down = deltas(owner)
        go(copies(("gy", 0, k), [ref_down], [y_down.at[place(k)]], side))
        go(copies(("gy", 1, k), [ref_gate_up], [y_gate_up.at[place(k)]], side))

    with jax.named_scope("wgrad_own"):

        @pl.loop(0, line)
        def _(t):
            weight_grads(t * 2 + y)

    wide = next(b for b in (512, 256, 128) if width % b == 0)

    @named
    def to_mate(i):
        go(copies(("pm", i), [part.at[i, :, other]], [part_in.at[i]], mate))

    @named
    def from_mate(i):
        arrived(("pm", i), [part_in.at[i]])

        @pl.loop(0, line)
        def _(t):
            here = block(t, rows, ROWS)
            add_strips(sums.at[i, t], part.at[i, here, mine], part_in.at[i, here, :])

    def add_in(i, t, key, landed):
        arrived((key, i, t), [landed.at[i, t]])
        add_strips(sums.at[i, t], sums.at[i, t], landed.at[i, t])

    @named
    def chain(i, stage):
        for here in range(line):
            up = [("zu", t, here + last - t) for t in range(last, here, -1)]
            low = [("zd", t, last - here + t) for t in range(here)]
            for key, t, when in sorted(up + low, key=lambda v: v[2]):
                first_hop = here == (0 if key == "zu" else last)
                if stage != (0 if first_hop else when):
                    continue
                landed, peer = (from_below, above) if key == "zu" else (from_above, below)
                if not first_hop:
                    on(z == here, functools.partial(add_in, i, t, key, landed))
                go(copies((key, i, t), [sums.at[i, t]], [landed.at[i, t]], peer), z == here)

    @named
    def finish(i):
        for t in range(line):
            if t > 0:
                on(z == t, functools.partial(add_in, i, t, "zu", from_below))
            if t < last:
                on(z == t, functools.partial(add_in, i, t, "zd", from_above))
        full[i, :, mine] = sums[i, z]
        go(copies(("fm", i), [full.at[i, :, mine]], [full.at[i, :, mine]], mate))

    @named
    def outputs():
        for i in range(2):
            arrived(("fm", i), [full.at[i, :, other]])

        @pl.loop(0, rows // ROWS)
        def _(j):
            here = block(j, ROWS, ROWS)
            late = x_late[here, :].astype(f32)
            out_late[here, :] = (late + 0.5 * full[0, here, :].astype(f32)).astype(bf16)
            early = x_early[here, :].astype(f32)
            scale = scale_of(early)
            unit = early * scale
            grad_normed = full[1, here, :].astype(f32)
            inner = jnp.mean(grad_normed * unit, axis=-1, keepdims=True)
            kept = acts[1, pl.ds(pl.multiple_of(z * rows + j * ROWS, ROWS), ROWS), :].astype(f32)
            grad_in[here, :] = (kept + scale * (grad_normed - unit * inner)).astype(bf16)

    @named
    def y_step(k, a):
        t = place(k)
        landed, went = (y_gate_up, x_gate_up) if a else (y_down, x_down)
        arrived(("gy", a, k), [landed.at[t]])
        add_strips(landed.at[t], deltas(t * 2 + y)[1 - a], landed.at[t])
        src = landed.at[t, block(1 - rep, deep if a else tall, ROWS), :]
        go(copies(("gx", a, k), [src], [went.at[t]], twin))

    def landing(place_of, who, a):
        at_rows, at_cols = block(who, deep, ROWS), block(place_of, layer, LANES)
        if a:
            return [delta_gate.at[at_rows, at_cols], delta_up.at[at_rows, at_cols]]
        return [delta_down.at[block(place_of * 2 + who, tall, ROWS), :]]

    puts = []

    @named
    def x_step(k, a):
        t = place(k)
        landed, kept = (x_gate_up, y_gate_up) if a else (x_down, y_down)
        arrived(("gx", a, k), [landed.at[t]])
        own = kept.at[t, block(rep, deep if a else tall, ROWS), :]
        add_strips(landed.at[t], own, landed.at[t])
        srcs = [landed.at[t]]
        if a:
            srcs = [landed.at[t, :, pl.ds(0, layer)], landed.at[t, :, pl.ds(layer, layer)]]
        to = landing(z, rep, a)
        if k:
            go(copies(("gz", a, k), srcs, to, {"fs": lax.rem(fs + 2 * k, n)}))
            return
        go(copies(("gt", a, 0), srcs, to, twin))
        for i, (s, d) in enumerate(zip(srcs, to)):
            put = pltpu.make_async_copy(s, d, local.at[a + i])
            put.start()
            puts.append(put)

    @named
    def z_step(k, a):
        refs = landing(origin(k), rep, a)
        arrived(("gz", a, k), refs)
        go(copies(("gt", a, k), refs, refs, twin))

    move(2, max(last - 2, 0))
    with jax.named_scope("norm_part"):

        @pl.loop(0, width // wide)
        def _(j):
            cols = block(j, wide, LANES)
            product = contract_cols(grads[...], gate_up[block(j, wide, ROWS), :])
            part[1, :, cols] = product.astype(bf16)

    to_mate(1)
    y_step(order[0], 0)
    from_mate(1)
    chain(1, 0)
    if last > 1:
        move(2, last - 1)
    y_step(order[0], 1)
    x_step(order[0], 0)
    for s in range(last):
        moved(2, s)
    with jax.named_scope("late_hidden"):

        @pl.loop(0, line)
        def _(t):
            here = block(t, rows, ROWS)
            hidden[here, :] = activations(acts[2, here, :])[3]

    x_step(order[0], 1)
    chain(1, 1)
    with jax.named_scope("late_part"):

        @pl.loop(0, width // wide)
        def _(j):
            cols = block(j, wide, LANES)
            product = jnp.dot(hidden[...], down[:, cols], preferred_element_type=f32)
            part[0, :, cols] = product.astype(bf16)

    to_mate(0)
    for stage in range(2, last):
        chain(1, stage)
    y_step(order[1], 0)
    from_mate(0)
    chain(0, 0)
    y_step(order[1], 1)
    for i in range(1, line):
        x_step(order[i], 0)
        if i == 1:
            finish(1)
        if i < last:
            x_step(order[i], 1)
            chain(0, i)
            for a in range(2):
                y_step(order[i + 1], a)
        else:
            finish(0)
            x_step(order[i], 1)
            outputs()
        for a in range(2):
            z_step(order[i - 1], a)
    with jax.named_scope("last_in"):
        for a in range(2):
            for k in order:
                arrived(("gt", a, k), landing(origin(k), 1 - rep, a))

    with jax.named_scope("drain"):
        for put in puts:
            put.wait()
        assert len(names) <= send.shape[0]
        for cond, group in pending:

            def drain():
                for copy in group:
                    copy.wait_send()

            if cond is None:
                drain()
            else:
                pl.when(cond)(drain)


def fast_shards(n, x_early, x_late, grad_out, w_gate, w_up, w_down, gate_sum, up_sum, down_sum):
    bf16 = jnp.bfloat16
    shape = jax.ShapeDtypeStruct
    line = n // 2
    rows, width = x_early.shape
    hidden_here, depth = w_down.shape
    layer = hidden_here // line
    tokens, half = line * rows, width // 2
    dma, vmem = pltpu.SemaphoreType.DMA, pl.BlockSpec(memory_space=pltpu.VMEM)
    count = 60 * line
    out_late, grad_in, delta_gate, delta_up, delta_down = pl.pallas_call(
        functools.partial(step_kernel, n),
        out_shape=[
            shape((rows, width), bf16),
            shape((rows, width), bf16),
            shape((depth, hidden_here), bf16),
            shape((depth, hidden_here), bf16),
            shape((hidden_here, depth), bf16),
        ],
        in_specs=[vmem, vmem, ANY, ANY, ANY, ANY],
        out_specs=[vmem, vmem, ANY, ANY, ANY],
        scratch_shapes=[
            pltpu.VMEM((3, tokens, width), bf16),
            pltpu.VMEM((width, 2 * layer), bf16),
            pltpu.VMEM((layer, width), bf16),
            pltpu.VMEM((tokens, layer), bf16),
            pltpu.VMEM((tokens, 2 * layer), bf16),
            pltpu.VMEM((2, tokens, width), bf16),
            pltpu.VMEM((2, tokens, half), bf16),
            pltpu.VMEM((2, line, rows, half), bf16),
            pltpu.VMEM((2, line, rows, half), bf16),
            pltpu.VMEM((2, line, rows, half), bf16),
            pltpu.VMEM((width, 2 * layer), bf16),
            pltpu.VMEM((layer, width), bf16),
            pltpu.VMEM((line, depth, 2 * layer), bf16),
            pltpu.VMEM((line, layer, depth), bf16),
            pltpu.VMEM((line, depth // 2, 2 * layer), bf16),
            pltpu.VMEM((line, layer // 2, depth), bf16),
            pltpu.VMEM((2, rows, width), bf16),
            dma((count,)),
            dma((count,)),
            dma((4,)),
        ],
        compiler_params=pltpu.CompilerParams(
            collective_id=0, has_side_effects=True, vmem_limit_bytes=56 * 2**20
        ),
    )(x_early, x_late, grad_out, w_gate, w_up, w_down)
    return (
        out_late,
        grad_in,
        gate_sum + delta_gate.astype(jnp.float32),
        up_sum + delta_up.astype(jnp.float32),
        down_sum + delta_down.astype(jnp.float32),
    )


def shards(x_early, x_late, grad_out, w_gate, w_up, w_down, gate_sum, up_sum, down_sum):
    gate_full, up_full, down_full = (
        lax.all_gather(w_gate, "fs", axis=0, tiled=True),
        lax.all_gather(w_up, "fs", axis=0, tiled=True),
        lax.all_gather(w_down, "fs", axis=1, tiled=True),
    )
    batch_rows = x_early.shape[0]
    stacked = jnp.concatenate([x_early, x_late], axis=0).astype(jnp.float32)
    row_scale = lax.rsqrt(jnp.mean(stacked * stacked, axis=-1, keepdims=True) + epsilon)
    normed = (stacked * row_scale).astype(jnp.bfloat16)
    gate_pre = jnp.dot(normed, gate_full, preferred_element_type=jnp.float32)
    up_pre = jnp.dot(normed, up_full, preferred_element_type=jnp.float32)
    gate_sig = jax.nn.sigmoid(gate_pre)
    hidden = (gate_pre * gate_sig * up_pre).astype(jnp.bfloat16)
    late_part = jnp.dot(hidden[batch_rows:], down_full, preferred_element_type=jnp.float32).astype(
        jnp.bfloat16
    )
    branch = lax.psum(late_part, "tp").astype(jnp.float32)
    out_late = (stacked[batch_rows:] + 0.5 * branch).astype(jnp.bfloat16)
    early_gate = gate_pre[:batch_rows]
    early_upper = up_pre[:batch_rows]
    early_sig = gate_sig[:batch_rows]
    early_hidden = hidden[:batch_rows]
    early_normed = normed[:batch_rows]
    early_scale = row_scale[:batch_rows]
    grad_hidden = 0.5 * contract_cols(grad_out, down_full)
    grad_gate_in = (
        grad_hidden * early_upper * early_sig * (1.0 + early_gate * (1.0 - early_sig))
    ).astype(jnp.bfloat16)
    grad_up_in = (grad_hidden * early_gate * early_sig).astype(jnp.bfloat16)
    normed_part = contract_cols(grad_gate_in, gate_full) + contract_cols(grad_up_in, up_full)
    grad_normed = lax.psum(normed_part.astype(jnp.bfloat16), "tp").astype(jnp.float32)
    unit_rows = stacked[:batch_rows] * early_scale
    inner = jnp.mean(grad_normed * unit_rows, axis=-1, keepdims=True)
    grad_in = (
        grad_out.astype(jnp.float32) + early_scale * (grad_normed - unit_rows * inner)
    ).astype(jnp.bfloat16)
    normed_cols, out_cols = (
        lax.all_to_all(early_normed, "fs", split_axis=1, concat_axis=0, tiled=True),
        lax.all_to_all(grad_out, "fs", split_axis=1, concat_axis=0, tiled=True),
    )
    gate_delta = contract_rows(normed_cols, lax.all_gather(grad_gate_in, "fs", axis=0, tiled=True))
    up_delta = contract_rows(normed_cols, lax.all_gather(grad_up_in, "fs", axis=0, tiled=True))
    down_half = contract_rows(lax.all_gather(early_hidden, "fs", axis=0, tiled=True), out_cols)
    down_delta = 0.5 * down_half
    gate_delta, up_delta, down_delta = (
        lax.psum(gate_delta.astype(jnp.bfloat16), "rep").astype(jnp.float32),
        lax.psum(up_delta.astype(jnp.bfloat16), "rep").astype(jnp.float32),
        lax.psum(down_delta.astype(jnp.bfloat16), "rep").astype(jnp.float32),
    )
    return (out_late, grad_in, gate_sum + gate_delta, up_sum + up_delta, down_sum + down_delta)


def shards_for(mesh):
    n, reps, cores = mesh.shape["fs"], mesh.shape["rep"], mesh.shape["tp"]

    def run(*args):
        rows, width = args[0].shape
        hidden_here, depth = args[5].shape
        line = max(n // 2, 1)
        layer = hidden_here // line
        fits = (
            reps == 2
            and cores == 2
            and n % 2 == 0
            and n >= 4
            and rows % ROWS == 0
            and width % (2 * LANES) == 0
            and depth % (2 * LANES) == 0
            and hidden_here % line == 0
            and layer % LANES == 0
            and layer % (2 * ROWS) == 0
            and 2 * (10 * line * rows * width + 10 * width * layer) < 44 * 2**20
        )
        return fast_shards(n, *args) if fits else shards(*args)

    return run


def solution(mesh):
    placed = (
        P(("rep", "fs"), None),
        P(("rep", "fs"), None),
        P(("rep", "fs"), None),
        P("fs", "tp"),
        P("fs", "tp"),
        P("tp", "fs"),
        P("fs", "tp"),
        P("fs", "tp"),
        P("tp", "fs"),
    )
    return jax.shard_map(
        shards_for(mesh),
        mesh=mesh,
        in_specs=placed,
        out_specs=(
            P(("rep", "fs"), None),
            P(("rep", "fs"), None),
            P("fs", "tp"),
            P("fs", "tp"),
            P("tp", "fs"),
        ),
        check_vma=False,
    )
```

```python
import functools

import jax
import jax.numpy as jnp
from jax import lax
from jax.experimental import pallas as pl
from jax.experimental.pallas import tpu as pltpu
from jax.sharding import PartitionSpec as P

epsilon = 1e-06
MESH = pl.DeviceIdType.MESH
ANY = pl.BlockSpec(memory_space=pl.ANY)
LANES, ROWS = 128, 16


def contract_rows(left, right):
    return lax.dot_general(
        left, right, (((0,), (0,)), ((), ())), preferred_element_type=jnp.float32
    )


def contract_cols(left, right):
    return lax.dot_general(
        left, right, (((1,), (1,)), ((), ())), preferred_element_type=jnp.float32
    )


def greet(peers):
    barrier = pltpu.get_barrier_semaphore()
    for peer in peers:
        pl.semaphore_signal(barrier, inc=1, device_id=peer, device_id_type=MESH)
    pl.semaphore_wait(barrier, len(peers))


def push(src, dst, send_sem, recv_sem, peer):
    copy = pltpu.make_async_remote_copy(
        src_ref=src,
        dst_ref=dst,
        send_sem=send_sem,
        recv_sem=recv_sem,
        device_id=peer,
        device_id_type=MESH,
    )
    return copy


def block(index, size, unit):
    return pl.ds(pl.multiple_of(index * size, unit), size)


def add_strips(dst, left, right):
    @pl.loop(0, dst.shape[0] // ROWS)
    def _(i):
        at = block(i, ROWS, ROWS)
        total = left[at, :].astype(jnp.float32) + right[at, :].astype(jnp.float32)
        dst[at, :] = total.astype(dst.dtype)


def named(f):
    def g(*args):
        tags = [str(a) for a in args if isinstance(a, int)]
        with jax.named_scope("_".join([f.__name__.strip("_")] + tags)):
            return f(*args)

    return g


def scale_of(v):
    return lax.rsqrt(jnp.mean(v * v, axis=-1, keepdims=True) + epsilon)


def step_kernel(
    n,
    early_in,
    late_in,
    grad_out,
    w_gate,
    w_up,
    w_down,
    out_late,
    grad_in,
    delta_gate,
    delta_up,
    delta_down,
    acts,
    gate_up,
    down,
    hidden,
    grads,
    part,
    part_in,
    sums,
    from_below,
    from_above,
    gate_up_delta,
    down_delta,
    y_gate_up,
    y_down,
    x_gate_up,
    x_down,
    a_gate_up,
    a_down,
    full,
    x_early,
    x_late,
    send,
    recv,
    local,
):
    f32, bf16 = jnp.float32, jnp.bfloat16
    rep, fs, tp = lax.axis_index("rep"), lax.axis_index("fs"), lax.axis_index("tp")
    line = n // 2
    z, y = fs // 2, lax.rem(fs, 2)
    twin, mate, side = {"rep": 1 - rep}, {"tp": 1 - tp}, {"fs": fs + 1 - 2 * y}
    above, below = {"fs": lax.rem(fs + 2, n)}, {"fs": lax.rem(fs + n - 2, n)}
    rows, width = x_early.shape
    layer, depth = down.shape[0], w_gate.shape[0]
    half, deep, tall = width // 2, depth // 2, layer // 2
    mine, other = block(tp, half, LANES), block(1 - tp, half, LANES)
    names, pending = {}, []
    last = line - 1
    wide = next(b for b in (512, 256, 128) if half % b == 0)

    def at(*key):
        return names.setdefault(key, len(names))

    def copies(key, srcs, dsts, peer):
        return [
            push(s, d, send.at[at(key, i)], recv.at[at(key, i)], peer)
            for i, (s, d) in enumerate(zip(srcs, dsts))
        ]

    def go(group, cond=None):
        def start():
            for copy in group:
                copy.start()

        pending.append((cond, group))
        if cond is None:
            start()
        else:
            pl.when(cond)(start)

    def arrived(key, refs):
        for copy in copies(key, refs, refs, twin):
            copy.wait_recv()

    def place(k):
        return lax.rem(z + k, line)

    def origin(k):
        return lax.rem(z + line - k, line)

    def slice3(owner, who):
        at_rows = block(owner * 2 + who, deep, ROWS)
        return [
            gate_up.at[at_rows, pl.ds(0, layer)],
            gate_up.at[at_rows, pl.ds(layer, layer)],
            down.at[block(who, tall, ROWS), block(owner, depth, LANES)],
        ]

    def slice2(owner, who):
        return [
            gate_up.at[block(owner * 2 + who, deep, ROWS), :],
            down.at[block(who, tall, ROWS), block(owner, depth, LANES)],
        ]

    def whole3(owner):
        at_rows = block(owner, depth, ROWS)
        return [
            gate_up.at[at_rows, pl.ds(0, layer)],
            gate_up.at[at_rows, pl.ds(layer, layer)],
            down.at[:, block(owner, depth, LANES)],
        ]

    def source3(to):
        at_rows, at_cols = block(rep, deep, ROWS), block(to, layer, LANES)
        return [
            w_gate.at[at_rows, at_cols],
            w_up.at[at_rows, at_cols],
            w_down.at[block(to * 2 + rep, tall, ROWS), :],
        ]

    own_source = [
        w_gate.at[:, block(z, layer, LANES)],
        w_up.at[:, block(z, layer, LANES)],
        w_down.at[block(z, layer, ROWS), :],
    ]
    own_rows = block(z, rows, ROWS)
    keeps = [
        pltpu.make_async_copy(s, d, local.at[i])
        for i, (s, d) in enumerate(zip(own_source, whole3(fs)))
    ]
    keeps.append(pltpu.make_async_copy(grad_out, acts.at[1, own_rows, :], local.at[3]))
    loads = [
        pltpu.make_async_copy(early_in, x_early, local.at[4]),
        pltpu.make_async_copy(late_in, x_late, local.at[5]),
    ]
    for keep in loads + keeps:
        keep.start()

    barrier = pltpu.get_barrier_semaphore()
    enter = jax.named_scope("enter")
    enter.__enter__()
    peers = [twin, mate, side] + [{"fs": lax.rem(fs + 2 * k, n)} for k in range(1, line)]
    for peer in peers:
        pl.semaphore_signal(barrier, inc=1, device_id=peer, device_id_type=MESH)
    pl.semaphore_wait(barrier, len(peers))
    enter.__exit__(None, None, None)

    def weights_out(d):
        up, low = {"fs": lax.rem(fs + 2 * d, n)}, {"fs": lax.rem(fs + n - 2 * d, n)}
        go(copies(("wu", d), source3(z + d), slice3(fs, rep), up), z + d < line)
        go(copies(("wd", d), source3(z - d), slice3(fs, rep), low), z - d >= 0)

    weights_out(1)
    go(copies("wy0", own_source, whole3(fs), side))

    @named
    def normalise(i, x):
        @pl.loop(0, rows // ROWS)
        def _(j):
            v = x[block(j, ROWS, ROWS), :].astype(f32)
            to = pl.ds(pl.multiple_of(z * rows + j * ROWS, ROWS), ROWS)
            acts[i, to, :] = (v * scale_of(v)).astype(bf16)

    def spot(i, place_of, cols=mine):
        return acts.at[i, block(place_of, rows, ROWS), cols]

    def go_up(i, s):
        src = grad_out.at[:, mine] if i == 1 and s == 0 else spot(i, z - s)
        go(copies(("up", i, s), [src], [spot(i, z - s)], above), (z - s >= 0) & (z < last))

    def go_down(i, s):
        src = grad_out.at[:, mine] if i == 1 and s == 0 else spot(i, z + s)
        go(copies(("down", i, s), [src], [spot(i, z + s)], below), (z + s < line) & (z > 0))

    @named
    def move(i, s):
        under, over = z - 1 - s, z + 1 + s
        pl.when(under >= 0)(lambda: arrived(("up", i, s), [spot(i, under)]))
        if s + 1 < last:
            go_up(i, s + 1)
        go(copies(("mu", i, s), [spot(i, under)], [spot(i, under)], mate), under >= 0)
        pl.when(over < line)(lambda: arrived(("down", i, s), [spot(i, over)]))
        if s + 1 < last:
            go_down(i, s + 1)
        go(copies(("md", i, s), [spot(i, over)], [spot(i, over)], mate), over < line)

    @named
    def moved(i, s):
        under, over = z - 1 - s, z + 1 + s
        pl.when(under >= 0)(lambda: arrived(("mu", i, s), [spot(i, under, other)]))
        pl.when(over < line)(lambda: arrived(("md", i, s), [spot(i, over, other)]))

    def first(i):
        go_up(i, 0)
        go_down(i, 0)

    for load in loads:
        load.wait()
    normalise(0, x_early)
    normalise(2, x_late)

    def layers(d):
        return (("wu", z - d, z - d >= 0), ("wd", z + d, z + d < line))

    def on(cond, f):
        pl.when(cond)(f)

    @named
    def weights_in(d):
        for tag, at_z, cond in layers(d):
            part2 = slice2(at_z * 2 + y, rep)
            on(cond, lambda: arrived((tag, d), slice3(at_z * 2 + y, rep)))
            go(copies((tag, "y", d), part2, part2, side), cond)
            go(copies((tag, "x", d), part2, part2, twin), cond)

    def turned(d):
        return d == 2

    @named
    def relay(d):
        for tag, at_z, cond in layers(d):
            if turned(d):
                part2, key, peer = slice2(at_z * 2 + y, 1 - rep), "x", side
            else:
                part2, key, peer = slice2(at_z * 2 + 1 - y, rep), "y", twin
            on(cond, lambda: arrived((tag, key, d), part2))
            go(copies((tag, "xy", d), part2, part2, peer), cond)

    @named
    def weights_done(d):
        for tag, at_z, cond in layers(d):
            if turned(d):
                part2, key = slice2(at_z * 2 + 1 - y, rep), "y"
            else:
                part2, key = slice2(at_z * 2 + y, 1 - rep), "x"
            on(cond, lambda: arrived((tag, key, d), part2))
            on(cond, lambda: arrived((tag, "xy", d), slice2(at_z * 2 + 1 - y, 1 - rep)))

    weights_in(1)
    for d in range(last, 1, -1):
        weights_out(d)
    first(1)
    first(0)
    for d in range(last, 2, -1):
        weights_in(d)
    relay(1)
    if line > 2:
        weights_in(2)
    for d in range(3, line):
        relay(d)
    for s in range(last - 1):
        move(1, s)
        move(0, s)
        if s == 0:
            relay(2)
    first(2)
    with jax.named_scope("weights_wait"):
        for keep in keeps:
            keep.wait()
        arrived("wy0", whole3(fs + 1 - 2 * y))
    for d in range(1, line):
        weights_done(d)

    def activations(x):
        pre = jnp.dot(x, gate_up[...], preferred_element_type=f32)
        g, u = pre[:, :layer], pre[:, layer:]
        s = jax.nn.sigmoid(g)
        return g, u, s, (g * s * u).astype(bf16)

    def early_block(place_of):
        here = block(place_of, rows, ROWS)
        g, u, s, h = activations(acts[0, here, :])
        grad_hidden = 0.5 * contract_cols(acts[1, here, :], down[...])
        hidden[here, :] = h
        grads[here, pl.ds(0, layer)] = (grad_hidden * u * s * (1.0 + g * (1.0 - s))).astype(bf16)
        grads[here, pl.ds(layer, layer)] = (grad_hidden * g * s).astype(bf16)

    with jax.named_scope("early_own"):
        early_block(z)
    for s in range(last):
        if s == last - 1:
            move(1, s)
            move(0, s)
        moved(1, s)
        moved(0, s)

        with jax.named_scope(f"early_{s}"):

            @pl.loop(0, 2)
            def _(d):
                to = z + (2 * d - 1) * (s + 1)
                pl.when((to >= 0) & (to < line))(lambda: early_block(to))

    order = list(range(1, line)) + [0]

    def weight_grads(owner):
        cols = block(owner, depth, LANES)
        gate_up_delta[block(owner, depth, ROWS), :] = contract_rows(
            acts[0, :, cols], grads[...]
        ).astype(bf16)
        down_delta[:, cols] = (0.5 * contract_rows(hidden[...], acts[1, :, cols])).astype(bf16)

    def deltas(owner):
        return [
            gate_up_delta.at[block(owner, depth, ROWS), :],
            down_delta.at[:, block(owner, depth, LANES)],
        ]

    lead = order[0]
    lead_z = place(lead)

    def lead_rows(who):
        return [
            gate_up_delta.at[block((lead_z * 2 + v) * 2 + who, deep, ROWS), :] for v in range(2)
        ]

    def lead_cols(who):
        return down_delta.at[block(who, tall, ROWS), block(lead_z, 2 * depth, LANES)]

    def y_send(k, a):
        src = deltas(place(k) * 2 + 1 - y)[1 - a]
        to = (y_gate_up if a else y_down).at[place(k)]
        go(copies(("gy", a, k), [src], [to], side))

    with jax.named_scope("wgrad_lead"):
        for v in range(2):
            weight_grads(lead_z * 2 + v)
    go(copies(("ax", 0), [lead_cols(1 - rep)], [a_down], twin))
    go(copies(("ax", 1), lead_rows(1 - rep), [a_gate_up.at[v] for v in range(2)], twin))
    for k in order[1:]:
        owner = place(k) * 2 + 1 - y
        with jax.named_scope(f"wgrad_{k}"):
            weight_grads(owner)
        if k == order[1]:
            y_send(k, 0)
            y_send(k, 1)

    @named
    def lead_x(a):
        if a:
            arrived(("ax", 1), [a_gate_up.at[v] for v in range(2)])
            for v, own in enumerate(lead_rows(rep)):
                add_strips(a_gate_up.at[v], own, a_gate_up.at[v])
            go(copies(("ay", 1), [a_gate_up.at[1 - y]], [x_gate_up.at[lead_z]], side))
            for k in order[2:3]:
                y_send(k, 1)
            for k in order[3:]:
                y_send(k, 0)
                y_send(k, 1)
        else:
            arrived(("ax", 0), [a_down])
            add_strips(a_down, lead_cols(rep), a_down)
            src = a_down.at[:, block(1 - y, depth, LANES)]
            go(copies(("ay", 0), [src], [x_down.at[lead_z]], side))
            for k in order[2:3]:
                y_send(k, 0)

    @named
    def to_mate(i):
        go(copies(("pm", i), [part.at[i, :, other]], [part_in.at[i]], mate))

    @named
    def from_mate(i):
        arrived(("pm", i), [part_in.at[i]])

        @pl.loop(0, line)
        def _(t):
            here = block(t, rows, ROWS)
            add_strips(sums.at[i, t], part.at[i, here, mine], part_in.at[i, here, :])

    def add_in(i, t, key, landed):
        arrived((key, i, t), [landed.at[i, t]])
        add_strips(sums.at[i, t], sums.at[i, t], landed.at[i, t])

    @named
    def chain(i, stage):
        for here in range(line):
            up = [("zu", t, here + last - t) for t in range(last, here, -1)]
            low = [("zd", t, last - here + t) for t in range(here)]
            for key, t, when in sorted(up + low, key=lambda v: v[2]):
                first_hop = here == (0 if key == "zu" else last)
                if stage != (max(when - 1, 0) if first_hop else when):
                    continue
                landed, peer = (from_below, above) if key == "zu" else (from_above, below)
                if not first_hop:
                    on(z == here, functools.partial(add_in, i, t, key, landed))
                go(copies((key, i, t), [sums.at[i, t]], [landed.at[i, t]], peer), z == here)

    @named
    def finish(i):
        for t in range(line):
            if t > 0:
                on(z == t, functools.partial(add_in, i, t, "zu", from_below))
            if t < last:
                on(z == t, functools.partial(add_in, i, t, "zd", from_above))
        full[i, :, mine] = sums[i, z]
        go(copies(("fm", i), [full.at[i, :, mine]], [full.at[i, :, mine]], mate))

    @named
    def output(i):
        arrived(("fm", i), [full.at[i, :, other]])

        @pl.loop(0, rows // ROWS)
        def _(j):
            here = block(j, ROWS, ROWS)
            total = full[i, here, :].astype(f32)
            if i == 0:
                late = x_late[here, :].astype(f32)
                out_late[here, :] = (late + 0.5 * total).astype(bf16)
                return
            early = x_early[here, :].astype(f32)
            scale = scale_of(early)
            unit = early * scale
            inner = jnp.mean(total * unit, axis=-1, keepdims=True)
            kept = acts[1, pl.ds(pl.multiple_of(z * rows + j * ROWS, ROWS), ROWS), :].astype(f32)
            grad_in[here, :] = (kept + scale * (total - unit * inner)).astype(bf16)

    @named
    def y_step(k, a):
        t = place(k)
        landed, went = (y_gate_up, x_gate_up) if a else (y_down, x_down)
        arrived(("gy", a, k), [landed.at[t]])
        add_strips(landed.at[t], deltas(t * 2 + y)[1 - a], landed.at[t])
        src = landed.at[t, block(1 - rep, deep if a else tall, ROWS), :]
        go(copies(("gx", a, k), [src], [went.at[t]], twin))

    def landing(place_of, who, a):
        at_rows, at_cols = block(who, deep, ROWS), block(place_of, layer, LANES)
        if a:
            return [delta_gate.at[at_rows, at_cols], delta_up.at[at_rows, at_cols]]
        return [delta_down.at[block(place_of * 2 + who, tall, ROWS), :]]

    puts = []

    @named
    def x_step(k, a):
        t = place(k)
        landed, kept = (x_gate_up, y_gate_up) if a else (x_down, y_down)
        if k == lead:
            arrived(("ay", a), [landed.at[t]])
            own = a_gate_up.at[y] if a else a_down.at[:, block(y, depth, LANES)]
        else:
            arrived(("gx", a, k), [landed.at[t]])
            own = kept.at[t, block(rep, deep if a else tall, ROWS), :]
        add_strips(landed.at[t], own, landed.at[t])
        srcs = [landed.at[t]]
        if a:
            srcs = [landed.at[t, :, pl.ds(0, layer)], landed.at[t, :, pl.ds(layer, layer)]]
        to = landing(z, rep, a)
        if k:
            go(copies(("gz", a, k), srcs, to, {"fs": lax.rem(fs + 2 * k, n)}))
            return
        go(copies(("gt", a, 0), srcs, to, twin))
        for i, (s, d) in enumerate(zip(srcs, to)):
            put = pltpu.make_async_copy(s, d, local.at[a + i])
            put.start()
            puts.append(put)

    @named
    def z_step(k, a):
        refs = landing(origin(k), rep, a)
        arrived(("gz", a, k), refs)
        go(copies(("gt", a, k), refs, refs, twin))

    def columns(i, who):
        @pl.loop(0, half // wide)
        def _(j):
            cols = block(who * (half // wide) + j, wide, LANES)
            if i:
                at_rows = block(who * (half // wide) + j, wide, ROWS)
                product = contract_cols(grads[...], gate_up[at_rows, :])
            else:
                product = jnp.dot(hidden[...], down[:, cols], preferred_element_type=f32)
            part[i, :, cols] = product.astype(bf16)

    @named
    def partials(i):
        columns(i, 1 - tp)
        to_mate(i)
        columns(i, tp)

    @named
    def late_hidden():
        for s in range(last):
            moved(2, s)

        @pl.loop(0, line)
        def _(t):
            here = block(t, rows, ROWS)
            hidden[here, :] = activations(acts[2, here, :])[3]

    for s in range(last - 2):
        move(2, s)
    partials(1)
    @named
    def wgrad_own():
        for k in order[1:]:
            weight_grads(place(k) * 2 + y)

    plan = ["a0", "w", "y20", "m", "c10", "v", "a1", "y21", "h", "x20", "x10", "c11", "p", "x21"]
    plan += ["y30", "n", "c00", "x11", "z10", "z20", "c12", "x30", "y31", "y00", "c01", "x31"]
    plan += ["z21", "f1", "x00", "y01", "z30", "c02", "z11", "x01", "o1", "z31", "f0", "o0"]
    if line != 4:
        plan = ["w", "m", "v", "h", "p", "n", "a0", "a1"]
        plan += [f"c{i}{stage}" for i in (1, 0) for stage in range(last)]
        plan += [f"y{k}{a}" for k in order[1:] for a in (0, 1)]
        plan += [f"{step}{k}{a}" for k in order for step in "xz" for a in (0, 1) if k or step < "z"]
        plan += ["f1", "f0", "o1", "o0"]
    steps = {"y": y_step, "x": x_step, "z": z_step, "c": chain}
    single = {
        "a0": lambda: lead_x(0),
        "a1": lambda: lead_x(1),
        "w": wgrad_own,
        "m": lambda: from_mate(1),
        "n": lambda: from_mate(0),
        "h": late_hidden,
        "p": lambda: partials(0),
        "f1": lambda: finish(1),
        "f0": lambda: finish(0),
        "o1": lambda: output(1),
        "o0": lambda: output(0),
    }

    def late_moves():
        for s in range(max(last - 2, 0), last):
            move(2, s)

    single["v"] = late_moves
    for name in plan:
        if name in single:
            single[name]()
        else:
            steps[name[0]](int(name[1]), int(name[2:]))
    with jax.named_scope("last_in"):
        for a in range(2):
            for k in order:
                arrived(("gt", a, k), landing(origin(k), 1 - rep, a))

    with jax.named_scope("drain"):
        for put in puts:
            put.wait()
        assert len(names) <= send.shape[0]
        for cond, group in pending:

            def drain():
                for copy in group:
                    copy.wait_send()

            if cond is None:
                drain()
            else:
                pl.when(cond)(drain)


def fast_shards(n, x_early, x_late, grad_out, w_gate, w_up, w_down, gate_sum, up_sum, down_sum):
    bf16 = jnp.bfloat16
    shape = jax.ShapeDtypeStruct
    line = n // 2
    rows, width = x_early.shape
    hidden_here, depth = w_down.shape
    layer = hidden_here // line
    tokens, half = line * rows, width // 2
    dma, vmem = pltpu.SemaphoreType.DMA, pl.BlockSpec(memory_space=pltpu.VMEM)
    count = 60 * line
    out_late, grad_in, delta_gate, delta_up, delta_down = pl.pallas_call(
        functools.partial(step_kernel, n),
        out_shape=[
            shape((rows, width), bf16),
            shape((rows, width), bf16),
            shape((depth, hidden_here), bf16),
            shape((depth, hidden_here), bf16),
            shape((hidden_here, depth), bf16),
        ],
        in_specs=[pl.BlockSpec(memory_space=pltpu.HBM)] * 6,
        out_specs=[vmem, vmem, ANY, ANY, ANY],
        scratch_shapes=[
            pltpu.VMEM((3, tokens, width), bf16),
            pltpu.VMEM((width, 2 * layer), bf16),
            pltpu.VMEM((layer, width), bf16),
            pltpu.VMEM((tokens, layer), bf16),
            pltpu.VMEM((tokens, 2 * layer), bf16),
            pltpu.VMEM((2, tokens, width), bf16),
            pltpu.VMEM((2, tokens, half), bf16),
            pltpu.VMEM((2, line, rows, half), bf16),
            pltpu.VMEM((2, line, rows, half), bf16),
            pltpu.VMEM((2, line, rows, half), bf16),
            pltpu.VMEM((width, 2 * layer), bf16),
            pltpu.VMEM((layer, width), bf16),
            pltpu.VMEM((line, depth, 2 * layer), bf16),
            pltpu.VMEM((line, layer, depth), bf16),
            pltpu.VMEM((line, depth // 2, 2 * layer), bf16),
            pltpu.VMEM((line, layer // 2, depth), bf16),
            pltpu.VMEM((2, depth // 2, 2 * layer), bf16),
            pltpu.VMEM((layer // 2, 2 * depth), bf16),
            pltpu.VMEM((2, rows, width), bf16),
            pltpu.VMEM((rows, width), bf16),
            pltpu.VMEM((rows, width), bf16),
            dma((count,)),
            dma((count,)),
            dma((6,)),
        ],
        compiler_params=pltpu.CompilerParams(
            collective_id=0, has_side_effects=True, vmem_limit_bytes=60 * 2**20
        ),
    )(x_early, x_late, grad_out, w_gate, w_up, w_down)
    return (
        out_late,
        grad_in,
        gate_sum + delta_gate.astype(jnp.float32),
        up_sum + delta_up.astype(jnp.float32),
        down_sum + delta_down.astype(jnp.float32),
    )


def shards(x_early, x_late, grad_out, w_gate, w_up, w_down, gate_sum, up_sum, down_sum):
    gate_full, up_full, down_full = (
        lax.all_gather(w_gate, "fs", axis=0, tiled=True),
        lax.all_gather(w_up, "fs", axis=0, tiled=True),
        lax.all_gather(w_down, "fs", axis=1, tiled=True),
    )
    batch_rows = x_early.shape[0]
    stacked = jnp.concatenate([x_early, x_late], axis=0).astype(jnp.float32)
    row_scale = lax.rsqrt(jnp.mean(stacked * stacked, axis=-1, keepdims=True) + epsilon)
    normed = (stacked * row_scale).astype(jnp.bfloat16)
    gate_pre = jnp.dot(normed, gate_full, preferred_element_type=jnp.float32)
    up_pre = jnp.dot(normed, up_full, preferred_element_type=jnp.float32)
    gate_sig = jax.nn.sigmoid(gate_pre)
    hidden = (gate_pre * gate_sig * up_pre).astype(jnp.bfloat16)
    late_part = jnp.dot(hidden[batch_rows:], down_full, preferred_element_type=jnp.float32).astype(
        jnp.bfloat16
    )
    branch = lax.psum(late_part, "tp").astype(jnp.float32)
    out_late = (stacked[batch_rows:] + 0.5 * branch).astype(jnp.bfloat16)
    early_gate = gate_pre[:batch_rows]
    early_upper = up_pre[:batch_rows]
    early_sig = gate_sig[:batch_rows]
    early_hidden = hidden[:batch_rows]
    early_normed = normed[:batch_rows]
    early_scale = row_scale[:batch_rows]
    grad_hidden = 0.5 * contract_cols(grad_out, down_full)
    grad_gate_in = (
        grad_hidden * early_upper * early_sig * (1.0 + early_gate * (1.0 - early_sig))
    ).astype(jnp.bfloat16)
    grad_up_in = (grad_hidden * early_gate * early_sig).astype(jnp.bfloat16)
    normed_part = contract_cols(grad_gate_in, gate_full) + contract_cols(grad_up_in, up_full)
    grad_normed = lax.psum(normed_part.astype(jnp.bfloat16), "tp").astype(jnp.float32)
    unit_rows = stacked[:batch_rows] * early_scale
    inner = jnp.mean(grad_normed * unit_rows, axis=-1, keepdims=True)
    grad_in = (
        grad_out.astype(jnp.float32) + early_scale * (grad_normed - unit_rows * inner)
    ).astype(jnp.bfloat16)
    normed_cols, out_cols = (
        lax.all_to_all(early_normed, "fs", split_axis=1, concat_axis=0, tiled=True),
        lax.all_to_all(grad_out, "fs", split_axis=1, concat_axis=0, tiled=True),
    )
    gate_delta = contract_rows(normed_cols, lax.all_gather(grad_gate_in, "fs", axis=0, tiled=True))
    up_delta = contract_rows(normed_cols, lax.all_gather(grad_up_in, "fs", axis=0, tiled=True))
    down_half = contract_rows(lax.all_gather(early_hidden, "fs", axis=0, tiled=True), out_cols)
    down_delta = 0.5 * down_half
    gate_delta, up_delta, down_delta = (
        lax.psum(gate_delta.astype(jnp.bfloat16), "rep").astype(jnp.float32),
        lax.psum(up_delta.astype(jnp.bfloat16), "rep").astype(jnp.float32),
        lax.psum(down_delta.astype(jnp.bfloat16), "rep").astype(jnp.float32),
    )
    return (out_late, grad_in, gate_sum + gate_delta, up_sum + up_delta, down_sum + down_delta)


def shards_for(mesh):
    n, reps, cores = mesh.shape["fs"], mesh.shape["rep"], mesh.shape["tp"]

    def run(*args):
        rows, width = args[0].shape
        hidden_here, depth = args[5].shape
        line = max(n // 2, 1)
        layer = hidden_here // line
        fits = (
            reps == 2
            and cores == 2
            and n % 2 == 0
            and n >= 4
            and rows % ROWS == 0
            and width % (2 * LANES) == 0
            and depth % (2 * LANES) == 0
            and hidden_here % line == 0
            and layer % LANES == 0
            and layer % (2 * ROWS) == 0
            and 2 * (10 * line * rows * width + 10 * width * layer) < 44 * 2**20
        )
        return fast_shards(n, *args) if fits else shards(*args)

    return run


def solution(mesh):
    placed = (
        P(("rep", "fs"), None),
        P(("rep", "fs"), None),
        P(("rep", "fs"), None),
        P("fs", "tp"),
        P("fs", "tp"),
        P("tp", "fs"),
        P("fs", "tp"),
        P("fs", "tp"),
        P("tp", "fs"),
    )
    return jax.shard_map(
        shards_for(mesh),
        mesh=mesh,
        in_specs=placed,
        out_specs=(
            P(("rep", "fs"), None),
            P(("rep", "fs"), None),
            P("fs", "tp"),
            P("fs", "tp"),
            P("tp", "fs"),
        ),
        check_vma=False,
    )
```

```python
import functools

import jax
import jax.numpy as jnp
from jax import lax
from jax.experimental import pallas as pl
from jax.experimental.pallas import tpu as pltpu
from jax.sharding import PartitionSpec as P

epsilon = 1e-06
MESH = pl.DeviceIdType.MESH
ANY = pl.BlockSpec(memory_space=pl.ANY)
LANES, ROWS = 128, 16


def contract_rows(left, right):
    return lax.dot_general(
        left, right, (((0,), (0,)), ((), ())), preferred_element_type=jnp.float32
    )


def contract_cols(left, right):
    return lax.dot_general(
        left, right, (((1,), (1,)), ((), ())), preferred_element_type=jnp.float32
    )


def greet(peers):
    barrier = pltpu.get_barrier_semaphore()
    for peer in peers:
        pl.semaphore_signal(barrier, inc=1, device_id=peer, device_id_type=MESH)
    pl.semaphore_wait(barrier, len(peers))


def push(src, dst, send_sem, recv_sem, peer):
    copy = pltpu.make_async_remote_copy(
        src_ref=src,
        dst_ref=dst,
        send_sem=send_sem,
        recv_sem=recv_sem,
        device_id=peer,
        device_id_type=MESH,
    )
    return copy


def block(index, size, unit):
    return pl.ds(pl.multiple_of(index * size, unit), size)


def add_strips(dst, left, right):
    @pl.loop(0, dst.shape[0] // ROWS)
    def _(i):
        at = block(i, ROWS, ROWS)
        total = left[at, :].astype(jnp.float32) + right[at, :].astype(jnp.float32)
        dst[at, :] = total.astype(dst.dtype)


def named(f):
    def g(*args):
        tags = [str(a) for a in args if isinstance(a, int)]
        with jax.named_scope("_".join([f.__name__.strip("_")] + tags)):
            return f(*args)

    return g


def scale_of(v):
    return lax.rsqrt(jnp.mean(v * v, axis=-1, keepdims=True) + epsilon)


def step_kernel(
    n,
    early_in,
    late_in,
    grad_out,
    w_gate,
    w_up,
    w_down,
    out_late,
    grad_in,
    delta_gate,
    delta_up,
    delta_down,
    acts,
    gate_up,
    down,
    hidden,
    grads,
    part,
    part_in,
    sums,
    from_below,
    from_above,
    gate_up_delta,
    down_delta,
    y_gate_up,
    y_down,
    x_gate_up,
    x_down,
    a_gate_up,
    a_down,
    full,
    x_early,
    x_late,
    send,
    recv,
    local,
):
    f32, bf16 = jnp.float32, jnp.bfloat16
    rep, fs, tp = lax.axis_index("rep"), lax.axis_index("fs"), lax.axis_index("tp")
    line = n // 2
    z, y = fs // 2, lax.rem(fs, 2)
    twin, mate, side = {"rep": 1 - rep}, {"tp": 1 - tp}, {"fs": fs + 1 - 2 * y}
    above, below = {"fs": lax.rem(fs + 2, n)}, {"fs": lax.rem(fs + n - 2, n)}
    rows, width = x_early.shape
    layer, depth = down.shape[0], w_gate.shape[0]
    half, deep, tall = width // 2, depth // 2, layer // 2
    mine, other = block(tp, half, LANES), block(1 - tp, half, LANES)
    names, pending, free, made = {}, [], [], []
    last = line - 1
    wide = next(b for b in (512, 256, 128) if half % b == 0)

    def at(*key):
        return names.setdefault(key, len(names))

    def send_index():
        if not free:
            made.append(len(made))
            return made[-1]
        return free.pop()

    def bytes_of(refs):
        if len(refs) == 1:
            return refs[0]
        total = sum(ref.shape[0] * ref.shape[1] for ref in refs)
        assert total % (2 * layer * ROWS) == 0
        return gate_up.at[pl.ds(0, total // (2 * layer)), :]

    def copies(key, srcs, dsts, peer):
        index = send_index()
        sems = send.at[index], recv.at[at(key)]
        return index, [push(s, d, *sems, peer) for s, d in zip(srcs, dsts)], bytes_of(dsts)

    def go(group, cond=None):
        def start():
            for copy in group[1]:
                copy.start()

        pending.append((cond, group))
        if cond is None:
            start()
        else:
            pl.when(cond)(start)

    def drain(groups):
        for cond, (index, _, ref) in groups:

            def wait():
                push(ref, ref, send.at[index], recv.at[0], twin).wait_send()

            if cond is None:
                wait()
            else:
                pl.when(cond)(wait)

    def arrived(key, refs):
        ref = bytes_of(refs)
        push(ref, ref, send.at[0], recv.at[at(key)], twin).wait_recv()

    def place(k):
        return lax.rem(z + k, line)

    def origin(k):
        return lax.rem(z + line - k, line)

    def slice3(owner, who):
        at_rows = block(owner * 2 + who, deep, ROWS)
        return [
            gate_up.at[at_rows, pl.ds(0, layer)],
            gate_up.at[at_rows, pl.ds(layer, layer)],
            down.at[block(who, tall, ROWS), block(owner, depth, LANES)],
        ]

    def slice2(owner, who):
        return [
            gate_up.at[block(owner * 2 + who, deep, ROWS), :],
            down.at[block(who, tall, ROWS), block(owner, depth, LANES)],
        ]

    def whole3(owner):
        at_rows = block(owner, depth, ROWS)
        return [
            gate_up.at[at_rows, pl.ds(0, layer)],
            gate_up.at[at_rows, pl.ds(layer, layer)],
            down.at[:, block(owner, depth, LANES)],
        ]

    def source3(to):
        at_rows, at_cols = block(rep, deep, ROWS), block(to, layer, LANES)
        return [
            w_gate.at[at_rows, at_cols],
            w_up.at[at_rows, at_cols],
            w_down.at[block(to * 2 + rep, tall, ROWS), :],
        ]

    own_source = [
        w_gate.at[:, block(z, layer, LANES)],
        w_up.at[:, block(z, layer, LANES)],
        w_down.at[block(z, layer, ROWS), :],
    ]
    own_rows = block(z, rows, ROWS)
    keeps = [
        pltpu.make_async_copy(s, d, local.at[i])
        for i, (s, d) in enumerate(zip(own_source, whole3(fs)))
    ]
    keeps.append(pltpu.make_async_copy(grad_out, acts.at[1, own_rows, :], local.at[3]))
    loads = [
        pltpu.make_async_copy(early_in, x_early, local.at[4]),
        pltpu.make_async_copy(late_in, x_late, local.at[5]),
    ]
    for keep in loads + keeps:
        keep.start()

    barrier = pltpu.get_barrier_semaphore()
    enter = jax.named_scope("enter")
    enter.__enter__()
    peers = [twin, mate, side] + [{"fs": lax.rem(fs + 2 * k, n)} for k in range(1, line)]
    for peer in peers:
        pl.semaphore_signal(barrier, inc=1, device_id=peer, device_id_type=MESH)
    pl.semaphore_wait(barrier, len(peers))
    enter.__exit__(None, None, None)

    def weights_out(d):
        up, low = {"fs": lax.rem(fs + 2 * d, n)}, {"fs": lax.rem(fs + n - 2 * d, n)}
        go(copies(("wu", d), source3(z + d), slice3(fs, rep), up), z + d < line)
        go(copies(("wd", d), source3(z - d), slice3(fs, rep), low), z - d >= 0)

    weights_out(1)
    go(copies("wy0", own_source, whole3(fs), side))

    @named
    def normalise(i, x):
        @pl.loop(0, rows // ROWS)
        def _(j):
            v = x[block(j, ROWS, ROWS), :].astype(f32)
            to = pl.ds(pl.multiple_of(z * rows + j * ROWS, ROWS), ROWS)
            acts[i, to, :] = (v * scale_of(v)).astype(bf16)

    def spot(i, place_of, cols=mine):
        return acts.at[i, block(place_of, rows, ROWS), cols]

    def go_up(i, s):
        src = grad_out.at[:, mine] if i == 1 and s == 0 else spot(i, z - s)
        go(copies(("up", i, s), [src], [spot(i, z - s)], above), (z - s >= 0) & (z < last))

    def go_down(i, s):
        src = grad_out.at[:, mine] if i == 1 and s == 0 else spot(i, z + s)
        go(copies(("down", i, s), [src], [spot(i, z + s)], below), (z + s < line) & (z > 0))

    @named
    def move(i, s):
        under, over = z - 1 - s, z + 1 + s
        pl.when(under >= 0)(lambda: arrived(("up", i, s), [spot(i, under)]))
        if s + 1 < last:
            go_up(i, s + 1)
        go(copies(("mu", i, s), [spot(i, under)], [spot(i, under)], mate), under >= 0)
        pl.when(over < line)(lambda: arrived(("down", i, s), [spot(i, over)]))
        if s + 1 < last:
            go_down(i, s + 1)
        go(copies(("md", i, s), [spot(i, over)], [spot(i, over)], mate), over < line)

    @named
    def moved(i, s):
        under, over = z - 1 - s, z + 1 + s
        pl.when(under >= 0)(lambda: arrived(("mu", i, s), [spot(i, under, other)]))
        pl.when(over < line)(lambda: arrived(("md", i, s), [spot(i, over, other)]))

    def first(i):
        go_up(i, 0)
        go_down(i, 0)

    for load in loads:
        load.wait()
    normalise(0, x_early)
    normalise(2, x_late)

    def layers(d):
        return (("wu", z - d, z - d >= 0), ("wd", z + d, z + d < line))

    def on(cond, f):
        pl.when(cond)(f)

    @named
    def weights_in(d):
        for tag, at_z, cond in layers(d):
            part2 = slice2(at_z * 2 + y, rep)
            on(cond, lambda: arrived((tag, d), slice3(at_z * 2 + y, rep)))
            go(copies((tag, "y", d), part2, part2, side), cond)
            go(copies((tag, "x", d), part2, part2, twin), cond)

    def turned(d):
        return d == 2

    @named
    def relay(d):
        for tag, at_z, cond in layers(d):
            if turned(d):
                part2, key, peer = slice2(at_z * 2 + y, 1 - rep), "x", side
            else:
                part2, key, peer = slice2(at_z * 2 + 1 - y, rep), "y", twin
            on(cond, lambda: arrived((tag, key, d), part2))
            go(copies((tag, "xy", d), part2, part2, peer), cond)

    @named
    def weights_done(d):
        for tag, at_z, cond in layers(d):
            if turned(d):
                part2, key = slice2(at_z * 2 + 1 - y, rep), "y"
            else:
                part2, key = slice2(at_z * 2 + y, 1 - rep), "x"
            on(cond, lambda: arrived((tag, key, d), part2))
            on(cond, lambda: arrived((tag, "xy", d), slice2(at_z * 2 + 1 - y, 1 - rep)))

    weights_in(1)
    for d in range(last, 1, -1):
        weights_out(d)
    first(1)
    first(0)
    for d in range(last, 2, -1):
        weights_in(d)
    if line > 2:
        weights_in(2)
    relay(1)
    for d in range(3, line):
        relay(d)
    for s in range(last - 1):
        move(1, s)
        move(0, s)
        if s == 0:
            relay(2)
    early_count = len(pending)
    first(2)
    with jax.named_scope("weights_wait"):
        for keep in keeps:
            keep.wait()
        arrived("wy0", whole3(fs + 1 - 2 * y))
    for d in range(1, line):
        weights_done(d)

    def activations(x):
        pre = jnp.dot(x, gate_up[...], preferred_element_type=f32)
        g, u = pre[:, :layer], pre[:, layer:]
        s = jax.nn.sigmoid(g)
        return g, u, s, (g * s * u).astype(bf16)

    def early_block(place_of):
        here = block(place_of, rows, ROWS)
        g, u, s, h = activations(acts[0, here, :])
        grad_hidden = 0.5 * contract_cols(acts[1, here, :], down[...])
        hidden[here, :] = h
        grads[here, pl.ds(0, layer)] = (grad_hidden * u * s * (1.0 + g * (1.0 - s))).astype(bf16)
        grads[here, pl.ds(layer, layer)] = (grad_hidden * g * s).astype(bf16)

    with jax.named_scope("early_own"):
        early_block(z)
    for s in range(last):
        if s == last - 1:
            move(1, s)
            move(0, s)
        moved(1, s)
        moved(0, s)

        with jax.named_scope(f"early_{s}"):

            @pl.loop(0, 2)
            def _(d):
                to = z + (2 * d - 1) * (s + 1)
                pl.when((to >= 0) & (to < line))(lambda: early_block(to))

    order = list(range(1, line)) + [0]

    def weight_grads(owner):
        cols = block(owner, depth, LANES)
        gate_up_delta[block(owner, depth, ROWS), :] = contract_rows(
            acts[0, :, cols], grads[...]
        ).astype(bf16)
        down_delta[:, cols] = (0.5 * contract_rows(hidden[...], acts[1, :, cols])).astype(bf16)

    def deltas(owner):
        return [
            gate_up_delta.at[block(owner, depth, ROWS), :],
            down_delta.at[:, block(owner, depth, LANES)],
        ]

    lead = order[0]
    lead_z = place(lead)

    def lead_rows(who):
        return [
            gate_up_delta.at[block((lead_z * 2 + v) * 2 + who, deep, ROWS), :] for v in range(2)
        ]

    def lead_cols(who):
        return down_delta.at[block(who, tall, ROWS), block(lead_z, 2 * depth, LANES)]

    def y_send(k, a):
        src = deltas(place(k) * 2 + 1 - y)[1 - a]
        to = (y_gate_up if a else y_down).at[place(k)]
        go(copies(("gy", a, k), [src], [to], side))

    with jax.named_scope("wgrad_lead"):
        for v in range(2):
            weight_grads(lead_z * 2 + v)
    go(copies(("ax", 0), [lead_cols(1 - rep)], [a_down], twin))
    go(copies(("ax", 1), lead_rows(1 - rep), [a_gate_up.at[v] for v in range(2)], twin))
    for k in order[1:]:
        owner = place(k) * 2 + 1 - y
        with jax.named_scope(f"wgrad_{k}"):
            weight_grads(owner)
        if k == order[1]:
            y_send(k, 0)
            y_send(k, 1)

    @named
    def lead_x(a):
        if a:
            arrived(("ax", 1), [a_gate_up.at[v] for v in range(2)])
            for v, own in enumerate(lead_rows(rep)):
                add_strips(a_gate_up.at[v], own, a_gate_up.at[v])
            go(copies(("ay", 1), [a_gate_up.at[1 - y]], [x_gate_up.at[lead_z]], side))
            for k in order[2:3]:
                y_send(k, 1)
            for k in order[3:]:
                y_send(k, 0)
                y_send(k, 1)
        else:
            arrived(("ax", 0), [a_down])
            add_strips(a_down, lead_cols(rep), a_down)
            src = a_down.at[:, block(1 - y, depth, LANES)]
            go(copies(("ay", 0), [src], [x_down.at[lead_z]], side))
            for k in order[2:3]:
                y_send(k, 0)

    @named
    def to_mate(i):
        go(copies(("pm", i), [part.at[i, :, other]], [part_in.at[i]], mate))

    @named
    def from_mate(i):
        arrived(("pm", i), [part_in.at[i]])

        @pl.loop(0, line)
        def _(t):
            here = block(t, rows, ROWS)
            add_strips(sums.at[i, t], part.at[i, here, mine], part_in.at[i, here, :])

    def add_in(i, t, key, landed):
        arrived((key, i, t), [landed.at[i, t]])
        add_strips(sums.at[i, t], sums.at[i, t], landed.at[i, t])

    @named
    def chain(i, stage):
        for here in range(line):
            up = [("zu", t, here + last - t) for t in range(last, here, -1)]
            low = [("zd", t, last - here + t) for t in range(here)]
            for key, t, when in sorted(up + low, key=lambda v: v[2]):
                first_hop = here == (0 if key == "zu" else last)
                if stage != when:
                    continue
                landed, peer = (from_below, above) if key == "zu" else (from_above, below)
                if not first_hop:
                    on(z == here, functools.partial(add_in, i, t, key, landed))
                go(copies((key, i, t), [sums.at[i, t]], [landed.at[i, t]], peer), z == here)

    @named
    def finish(i):
        for t in range(line):
            if t > 0:
                on(z == t, functools.partial(add_in, i, t, "zu", from_below))
            if t < last:
                on(z == t, functools.partial(add_in, i, t, "zd", from_above))
        full[i, :, mine] = sums[i, z]
        go(copies(("fm", i), [full.at[i, :, mine]], [full.at[i, :, mine]], mate))

    @named
    def output(i):
        arrived(("fm", i), [full.at[i, :, other]])

        @pl.loop(0, rows // ROWS)
        def _(j):
            here = block(j, ROWS, ROWS)
            total = full[i, here, :].astype(f32)
            if i == 0:
                late = x_late[here, :].astype(f32)
                out_late[here, :] = (late + 0.5 * total).astype(bf16)
                return
            early = x_early[here, :].astype(f32)
            scale = scale_of(early)
            unit = early * scale
            inner = jnp.mean(total * unit, axis=-1, keepdims=True)
            kept = acts[1, pl.ds(pl.multiple_of(z * rows + j * ROWS, ROWS), ROWS), :].astype(f32)
            grad_in[here, :] = (kept + scale * (total - unit * inner)).astype(bf16)

    @named
    def y_step(k, a):
        t = place(k)
        landed, went = (y_gate_up, x_gate_up) if a else (y_down, x_down)
        arrived(("gy", a, k), [landed.at[t]])
        add_strips(landed.at[t], deltas(t * 2 + y)[1 - a], landed.at[t])
        src = landed.at[t, block(1 - rep, deep if a else tall, ROWS), :]
        go(copies(("gx", a, k), [src], [went.at[t]], twin))

    def landing(place_of, who, a):
        at_rows, at_cols = block(who, deep, ROWS), block(place_of, layer, LANES)
        if a:
            return [delta_gate.at[at_rows, at_cols], delta_up.at[at_rows, at_cols]]
        return [delta_down.at[block(place_of * 2 + who, tall, ROWS), :]]

    puts = []

    @named
    def x_step(k, a):
        t = place(k)
        landed, kept = (x_gate_up, y_gate_up) if a else (x_down, y_down)
        if k == lead:
            arrived(("ay", a), [landed.at[t]])
            own = a_gate_up.at[y] if a else a_down.at[:, block(y, depth, LANES)]
        else:
            arrived(("gx", a, k), [landed.at[t]])
            own = kept.at[t, block(rep, deep if a else tall, ROWS), :]
        add_strips(landed.at[t], own, landed.at[t])
        srcs = [landed.at[t]]
        if a:
            srcs = [landed.at[t, :, pl.ds(0, layer)], landed.at[t, :, pl.ds(layer, layer)]]
        to = landing(z, rep, a)
        if k:
            go(copies(("gz", a, k), srcs, to, {"fs": lax.rem(fs + 2 * k, n)}))
            return
        go(copies(("gt", a, 0), srcs, to, twin))
        for i, (s, d) in enumerate(zip(srcs, to)):
            put = pltpu.make_async_copy(s, d, local.at[a + i])
            put.start()
            puts.append(put)

    @named
    def z_step(k, a):
        refs = landing(origin(k), rep, a)
        arrived(("gz", a, k), refs)
        go(copies(("gt", a, k), refs, refs, twin))

    def columns(i, who):
        @pl.loop(0, half // wide)
        def _(j):
            cols = block(who * (half // wide) + j, wide, LANES)
            if i:
                at_rows = block(who * (half // wide) + j, wide, ROWS)
                product = contract_cols(grads[...], gate_up[at_rows, :])
            else:
                product = jnp.dot(hidden[...], down[:, cols], preferred_element_type=f32)
            part[i, :, cols] = product.astype(bf16)

    @named
    def partials(i):
        columns(i, 1 - tp)
        to_mate(i)
        columns(i, tp)

    @named
    def late_hidden():
        for s in range(last):
            moved(2, s)

        @pl.loop(0, line)
        def _(t):
            here = block(t, rows, ROWS)
            hidden[here, :] = activations(acts[2, here, :])[3]

    for s in range(last - 2):
        move(2, s)
    partials(1)
    with jax.named_scope("recycle"):
        drain(pending[:early_count])
        free.extend(group[0] for _, group in pending[:early_count])
        del pending[:early_count]

    @named
    def wgrad_own():
        for k in order[1:]:
            weight_grads(place(k) * 2 + y)

    plan = ["a0", "w", "y20", "m", "c10", "v", "a1", "y21", "h", "x20", "x10", "c11", "p", "x21"]
    plan += ["y30", "n", "c00", "x11", "z10", "z20", "c12", "x30", "y31", "y00", "c01", "x31"]
    plan += ["z21", "x00", "y01", "z11", "z30", "f1", "x01", "c02", "z31", "o1", "f0", "o0"]
    if line != 4:
        plan = ["w", "m", "v", "h", "p", "n", "a0", "a1"]
        plan += [f"c{i}{stage}" for i in (1, 0) for stage in range(last)]
        plan += [f"y{k}{a}" for k in order[1:] for a in (0, 1)]
        plan += [f"{step}{k}{a}" for k in order for step in "xz" for a in (0, 1) if k or step < "z"]
        plan += ["f1", "f0", "o1", "o0"]
    steps = {"y": y_step, "x": x_step, "z": z_step, "c": chain}
    single = {
        "a0": lambda: lead_x(0),
        "a1": lambda: lead_x(1),
        "w": wgrad_own,
        "m": lambda: from_mate(1),
        "n": lambda: from_mate(0),
        "h": late_hidden,
        "p": lambda: partials(0),
        "f1": lambda: finish(1),
        "f0": lambda: finish(0),
        "o1": lambda: output(1),
        "o0": lambda: output(0),
    }

    def late_moves():
        for s in range(max(last - 2, 0), last):
            move(2, s)

    single["v"] = late_moves
    for name in plan:
        if name in single:
            single[name]()
        else:
            steps[name[0]](int(name[1]), int(name[2:]))
    with jax.named_scope("last_in"):
        for a in range(2):
            for k in order:
                arrived(("gt", a, k), landing(origin(k), 1 - rep, a))

    with jax.named_scope("drain"):
        for put in puts:
            put.wait()
        assert len(names) <= recv.shape[0] and len(made) <= send.shape[0]
        drain(pending)


def fast_shards(n, x_early, x_late, grad_out, w_gate, w_up, w_down, gate_sum, up_sum, down_sum):
    bf16 = jnp.bfloat16
    shape = jax.ShapeDtypeStruct
    line = n // 2
    rows, width = x_early.shape
    hidden_here, depth = w_down.shape
    layer = hidden_here // line
    tokens, half = line * rows, width // 2
    dma, vmem = pltpu.SemaphoreType.DMA, pl.BlockSpec(memory_space=pltpu.VMEM)
    out_late, grad_in, delta_gate, delta_up, delta_down = pl.pallas_call(
        functools.partial(step_kernel, n),
        out_shape=[
            shape((rows, width), bf16),
            shape((rows, width), bf16),
            shape((depth, hidden_here), bf16),
            shape((depth, hidden_here), bf16),
            shape((hidden_here, depth), bf16),
        ],
        in_specs=[pl.BlockSpec(memory_space=pltpu.HBM)] * 6,
        out_specs=[vmem, vmem, ANY, ANY, ANY],
        scratch_shapes=[
            pltpu.VMEM((3, tokens, width), bf16),
            pltpu.VMEM((width, 2 * layer), bf16),
            pltpu.VMEM((layer, width), bf16),
            pltpu.VMEM((tokens, layer), bf16),
            pltpu.VMEM((tokens, 2 * layer), bf16),
            pltpu.VMEM((2, tokens, width), bf16),
            pltpu.VMEM((2, tokens, half), bf16),
            pltpu.VMEM((2, line, rows, half), bf16),
            pltpu.VMEM((2, line, rows, half), bf16),
            pltpu.VMEM((2, line, rows, half), bf16),
            pltpu.VMEM((width, 2 * layer), bf16),
            pltpu.VMEM((layer, width), bf16),
            pltpu.VMEM((line, depth, 2 * layer), bf16),
            pltpu.VMEM((line, layer, depth), bf16),
            pltpu.VMEM((line, depth // 2, 2 * layer), bf16),
            pltpu.VMEM((line, layer // 2, depth), bf16),
            pltpu.VMEM((2, depth // 2, 2 * layer), bf16),
            pltpu.VMEM((layer // 2, 2 * depth), bf16),
            pltpu.VMEM((2, rows, width), bf16),
            pltpu.VMEM((rows, width), bf16),
            pltpu.VMEM((rows, width), bf16),
            dma((22 * line - 14,)),
            dma((32 * line - 21,)),
            dma((6,)),
        ],
        compiler_params=pltpu.CompilerParams(
            collective_id=0, has_side_effects=True, vmem_limit_bytes=60 * 2**20
        ),
    )(x_early, x_late, grad_out, w_gate, w_up, w_down)
    return (
        out_late,
        grad_in,
        gate_sum + delta_gate.astype(jnp.float32),
        up_sum + delta_up.astype(jnp.float32),
        down_sum + delta_down.astype(jnp.float32),
    )


def shards(x_early, x_late, grad_out, w_gate, w_up, w_down, gate_sum, up_sum, down_sum):
    gate_full, up_full, down_full = (
        lax.all_gather(w_gate, "fs", axis=0, tiled=True),
        lax.all_gather(w_up, "fs", axis=0, tiled=True),
        lax.all_gather(w_down, "fs", axis=1, tiled=True),
    )
    batch_rows = x_early.shape[0]
    stacked = jnp.concatenate([x_early, x_late], axis=0).astype(jnp.float32)
    row_scale = lax.rsqrt(jnp.mean(stacked * stacked, axis=-1, keepdims=True) + epsilon)
    normed = (stacked * row_scale).astype(jnp.bfloat16)
    gate_pre = jnp.dot(normed, gate_full, preferred_element_type=jnp.float32)
    up_pre = jnp.dot(normed, up_full, preferred_element_type=jnp.float32)
    gate_sig = jax.nn.sigmoid(gate_pre)
    hidden = (gate_pre * gate_sig * up_pre).astype(jnp.bfloat16)
    late_part = jnp.dot(hidden[batch_rows:], down_full, preferred_element_type=jnp.float32).astype(
        jnp.bfloat16
    )
    branch = lax.psum(late_part, "tp").astype(jnp.float32)
    out_late = (stacked[batch_rows:] + 0.5 * branch).astype(jnp.bfloat16)
    early_gate = gate_pre[:batch_rows]
    early_upper = up_pre[:batch_rows]
    early_sig = gate_sig[:batch_rows]
    early_hidden = hidden[:batch_rows]
    early_normed = normed[:batch_rows]
    early_scale = row_scale[:batch_rows]
    grad_hidden = 0.5 * contract_cols(grad_out, down_full)
    grad_gate_in = (
        grad_hidden * early_upper * early_sig * (1.0 + early_gate * (1.0 - early_sig))
    ).astype(jnp.bfloat16)
    grad_up_in = (grad_hidden * early_gate * early_sig).astype(jnp.bfloat16)
    normed_part = contract_cols(grad_gate_in, gate_full) + contract_cols(grad_up_in, up_full)
    grad_normed = lax.psum(normed_part.astype(jnp.bfloat16), "tp").astype(jnp.float32)
    unit_rows = stacked[:batch_rows] * early_scale
    inner = jnp.mean(grad_normed * unit_rows, axis=-1, keepdims=True)
    grad_in = (
        grad_out.astype(jnp.float32) + early_scale * (grad_normed - unit_rows * inner)
    ).astype(jnp.bfloat16)
    normed_cols, out_cols = (
        lax.all_to_all(early_normed, "fs", split_axis=1, concat_axis=0, tiled=True),
        lax.all_to_all(grad_out, "fs", split_axis=1, concat_axis=0, tiled=True),
    )
    gate_delta = contract_rows(normed_cols, lax.all_gather(grad_gate_in, "fs", axis=0, tiled=True))
    up_delta = contract_rows(normed_cols, lax.all_gather(grad_up_in, "fs", axis=0, tiled=True))
    down_half = contract_rows(lax.all_gather(early_hidden, "fs", axis=0, tiled=True), out_cols)
    down_delta = 0.5 * down_half
    gate_delta, up_delta, down_delta = (
        lax.psum(gate_delta.astype(jnp.bfloat16), "rep").astype(jnp.float32),
        lax.psum(up_delta.astype(jnp.bfloat16), "rep").astype(jnp.float32),
        lax.psum(down_delta.astype(jnp.bfloat16), "rep").astype(jnp.float32),
    )
    return (out_late, grad_in, gate_sum + gate_delta, up_sum + up_delta, down_sum + down_delta)


def shards_for(mesh):
    n, reps, cores = mesh.shape["fs"], mesh.shape["rep"], mesh.shape["tp"]

    def run(*args):
        rows, width = args[0].shape
        hidden_here, depth = args[5].shape
        line = max(n // 2, 1)
        layer = hidden_here // line
        fits = (
            reps == 2
            and cores == 2
            and n % 2 == 0
            and n >= 4
            and rows % ROWS == 0
            and width % (2 * LANES) == 0
            and depth % (2 * LANES) == 0
            and hidden_here % line == 0
            and layer % LANES == 0
            and layer % (2 * ROWS) == 0
            and 2 * (10 * line * rows * width + 10 * width * layer) < 44 * 2**20
        )
        return fast_shards(n, *args) if fits else shards(*args)

    return run


def solution(mesh):
    placed = (
        P(("rep", "fs"), None),
        P(("rep", "fs"), None),
        P(("rep", "fs"), None),
        P("fs", "tp"),
        P("fs", "tp"),
        P("tp", "fs"),
        P("fs", "tp"),
        P("fs", "tp"),
        P("tp", "fs"),
    )
    return jax.shard_map(
        shards_for(mesh),
        mesh=mesh,
        in_specs=placed,
        out_specs=(
            P(("rep", "fs"), None),
            P(("rep", "fs"), None),
            P("fs", "tp"),
            P("fs", "tp"),
            P("tp", "fs"),
        ),
        check_vma=False,
    )
```

```python
import functools

import jax
import jax.numpy as jnp
from jax import lax
from jax.experimental import pallas as pl
from jax.experimental.pallas import tpu as pltpu
from jax.sharding import PartitionSpec as P

epsilon = 1e-06
MESH = pl.DeviceIdType.MESH
ANY = pl.BlockSpec(memory_space=pl.ANY)
LANES, ROWS = 128, 16


def contract_rows(left, right):
    return lax.dot_general(
        left, right, (((0,), (0,)), ((), ())), preferred_element_type=jnp.float32
    )


def contract_cols(left, right):
    return lax.dot_general(
        left, right, (((1,), (1,)), ((), ())), preferred_element_type=jnp.float32
    )


def greet(peers):
    barrier = pltpu.get_barrier_semaphore()
    for peer in peers:
        pl.semaphore_signal(barrier, inc=1, device_id=peer, device_id_type=MESH)
    pl.semaphore_wait(barrier, len(peers))


def push(src, dst, send_sem, recv_sem, peer):
    copy = pltpu.make_async_remote_copy(
        src_ref=src,
        dst_ref=dst,
        send_sem=send_sem,
        recv_sem=recv_sem,
        device_id=peer,
        device_id_type=MESH,
    )
    return copy


def block(index, size, unit):
    return pl.ds(pl.multiple_of(index * size, unit), size)


def add_strips(dst, left, right):
    @pl.loop(0, dst.shape[0] // ROWS)
    def _(i):
        at = block(i, ROWS, ROWS)
        total = left[at, :].astype(jnp.float32) + right[at, :].astype(jnp.float32)
        dst[at, :] = total.astype(dst.dtype)


def named(f):
    def g(*args):
        tags = [str(a) for a in args if isinstance(a, int)]
        with jax.named_scope("_".join([f.__name__.strip("_")] + tags)):
            return f(*args)

    return g


def scale_of(v):
    return lax.rsqrt(jnp.mean(v * v, axis=-1, keepdims=True) + epsilon)


def step_kernel(
    n,
    early_in,
    late_in,
    grad_out,
    w_gate,
    w_up,
    w_down,
    out_late,
    grad_in,
    delta_gate,
    delta_up,
    delta_down,
    acts,
    gate_up,
    down,
    hidden,
    grads,
    part,
    part_in,
    sums,
    from_below,
    from_above,
    gate_up_delta,
    down_delta,
    y_gate_up,
    y_down,
    x_gate_up,
    x_down,
    a_gate_up,
    a_down,
    full,
    x_early,
    x_late,
    send,
    recv,
    local,
):
    f32, bf16 = jnp.float32, jnp.bfloat16
    rep, fs, tp = lax.axis_index("rep"), lax.axis_index("fs"), lax.axis_index("tp")
    line = n // 2
    z, y = fs // 2, lax.rem(fs, 2)
    twin, mate, side = {"rep": 1 - rep}, {"tp": 1 - tp}, {"fs": fs + 1 - 2 * y}
    above, below = {"fs": lax.rem(fs + 2, n)}, {"fs": lax.rem(fs + n - 2, n)}
    rows, width = x_early.shape
    layer, depth = down.shape[0], w_gate.shape[0]
    half, deep, tall = width // 2, depth // 2, layer // 2
    mine, other = block(tp, half, LANES), block(1 - tp, half, LANES)
    names, pending, free, made = {}, [], [], []
    last = line - 1
    wide = next(b for b in (512, 256, 128) if half % b == 0)

    def at(*key):
        return names.setdefault(key, len(names))

    def send_index():
        if not free:
            made.append(len(made))
            return made[-1]
        return free.pop()

    def bytes_of(refs):
        if len(refs) == 1:
            return refs[0]
        total = sum(ref.shape[0] * ref.shape[1] for ref in refs)
        assert total % (2 * layer * ROWS) == 0
        return gate_up.at[pl.ds(0, total // (2 * layer)), :]

    def copies(key, srcs, dsts, peer):
        index = send_index()
        sems = send.at[index], recv.at[at(key)]
        return index, [push(s, d, *sems, peer) for s, d in zip(srcs, dsts)], bytes_of(dsts)

    def go(group, cond=None):
        def start():
            for copy in group[1]:
                copy.start()

        pending.append((cond, group))
        if cond is None:
            start()
        else:
            pl.when(cond)(start)

    def drain(groups):
        for cond, (index, _, ref) in groups:

            def wait():
                push(ref, ref, send.at[index], recv.at[0], twin).wait_send()

            if cond is None:
                wait()
            else:
                pl.when(cond)(wait)

    def arrived(key, refs):
        ref = bytes_of(refs)
        push(ref, ref, send.at[0], recv.at[at(key)], twin).wait_recv()

    def place(k):
        return lax.rem(z + k, line)

    def origin(k):
        return lax.rem(z + line - k, line)

    def slice3(owner, who):
        at_rows = block(owner * 2 + who, deep, ROWS)
        return [
            gate_up.at[at_rows, pl.ds(0, layer)],
            gate_up.at[at_rows, pl.ds(layer, layer)],
            down.at[block(who, tall, ROWS), block(owner, depth, LANES)],
        ]

    def slice2(owner, who):
        return [
            gate_up.at[block(owner * 2 + who, deep, ROWS), :],
            down.at[block(who, tall, ROWS), block(owner, depth, LANES)],
        ]

    def whole3(owner):
        at_rows = block(owner, depth, ROWS)
        return [
            gate_up.at[at_rows, pl.ds(0, layer)],
            gate_up.at[at_rows, pl.ds(layer, layer)],
            down.at[:, block(owner, depth, LANES)],
        ]

    def source3(to):
        at_rows, at_cols = block(rep, deep, ROWS), block(to, layer, LANES)
        return [
            w_gate.at[at_rows, at_cols],
            w_up.at[at_rows, at_cols],
            w_down.at[block(to * 2 + rep, tall, ROWS), :],
        ]

    own_source = [
        w_gate.at[:, block(z, layer, LANES)],
        w_up.at[:, block(z, layer, LANES)],
        w_down.at[block(z, layer, ROWS), :],
    ]
    own_rows = block(z, rows, ROWS)
    keeps = [
        pltpu.make_async_copy(s, d, local.at[i])
        for i, (s, d) in enumerate(zip(own_source, whole3(fs)))
    ]
    keeps.append(pltpu.make_async_copy(grad_out, acts.at[1, own_rows, :], local.at[3]))
    loads = [
        pltpu.make_async_copy(early_in, x_early, local.at[4]),
        pltpu.make_async_copy(late_in, x_late, local.at[5]),
    ]
    for keep in loads + keeps:
        keep.start()

    barrier = pltpu.get_barrier_semaphore()
    enter = jax.named_scope("enter")
    enter.__enter__()
    peers = [twin, mate, side] + [{"fs": lax.rem(fs + 2 * k, n)} for k in range(1, line)]
    for peer in peers:
        pl.semaphore_signal(barrier, inc=1, device_id=peer, device_id_type=MESH)
    pl.semaphore_wait(barrier, len(peers))
    enter.__exit__(None, None, None)

    def weights_out(d):
        up, low = {"fs": lax.rem(fs + 2 * d, n)}, {"fs": lax.rem(fs + n - 2 * d, n)}
        go(copies(("wu", d), source3(z + d), slice3(fs, rep), up), z + d < line)
        go(copies(("wd", d), source3(z - d), slice3(fs, rep), low), z - d >= 0)

    weights_out(1)
    go(copies("wy0", own_source, whole3(fs), side))

    @named
    def normalise(i, x):
        @pl.loop(0, rows // ROWS)
        def _(j):
            v = x[block(j, ROWS, ROWS), :].astype(f32)
            to = pl.ds(pl.multiple_of(z * rows + j * ROWS, ROWS), ROWS)
            acts[i, to, :] = (v * scale_of(v)).astype(bf16)

    def spot(i, place_of, cols=mine):
        return acts.at[i, block(place_of, rows, ROWS), cols]

    def go_up(i, s):
        src = grad_out.at[:, mine] if i == 1 and s == 0 else spot(i, z - s)
        go(copies(("up", i, s), [src], [spot(i, z - s)], above), (z - s >= 0) & (z < last))

    def go_down(i, s):
        src = grad_out.at[:, mine] if i == 1 and s == 0 else spot(i, z + s)
        go(copies(("down", i, s), [src], [spot(i, z + s)], below), (z + s < line) & (z > 0))

    @named
    def move(i, s):
        under, over = z - 1 - s, z + 1 + s
        pl.when(under >= 0)(lambda: arrived(("up", i, s), [spot(i, under)]))
        if s + 1 < last:
            go_up(i, s + 1)
        go(copies(("mu", i, s), [spot(i, under)], [spot(i, under)], mate), under >= 0)
        pl.when(over < line)(lambda: arrived(("down", i, s), [spot(i, over)]))
        if s + 1 < last:
            go_down(i, s + 1)
        go(copies(("md", i, s), [spot(i, over)], [spot(i, over)], mate), over < line)

    @named
    def moved(i, s):
        under, over = z - 1 - s, z + 1 + s
        pl.when(under >= 0)(lambda: arrived(("mu", i, s), [spot(i, under, other)]))
        pl.when(over < line)(lambda: arrived(("md", i, s), [spot(i, over, other)]))

    def first(i):
        go_up(i, 0)
        go_down(i, 0)

    for load in loads:
        load.wait()
    normalise(0, x_early)
    normalise(2, x_late)

    def layers(d):
        return (("wu", z - d, z - d >= 0), ("wd", z + d, z + d < line))

    def on(cond, f):
        pl.when(cond)(f)

    @named
    def weights_in(d):
        for tag, at_z, cond in layers(d):
            part2 = slice2(at_z * 2 + y, rep)
            on(cond, lambda: arrived((tag, d), slice3(at_z * 2 + y, rep)))
            go(copies((tag, "y", d), part2, part2, side), cond)
            go(copies((tag, "x", d), part2, part2, twin), cond)

    def turned(d):
        return d == 2

    @named
    def relay(d):
        for tag, at_z, cond in layers(d):
            if turned(d):
                part2, key, peer = slice2(at_z * 2 + y, 1 - rep), "x", side
            else:
                part2, key, peer = slice2(at_z * 2 + 1 - y, rep), "y", twin
            on(cond, lambda: arrived((tag, key, d), part2))
            go(copies((tag, "xy", d), part2, part2, peer), cond)

    @named
    def weights_done(d):
        for tag, at_z, cond in layers(d):
            if turned(d):
                part2, key = slice2(at_z * 2 + 1 - y, rep), "y"
            else:
                part2, key = slice2(at_z * 2 + y, 1 - rep), "x"
            on(cond, lambda: arrived((tag, key, d), part2))
            on(cond, lambda: arrived((tag, "xy", d), slice2(at_z * 2 + 1 - y, 1 - rep)))

    weights_in(1)
    for d in range(last, 1, -1):
        weights_out(d)
    first(1)
    first(0)
    for d in range(last, 2, -1):
        weights_in(d)
    if line > 2:
        weights_in(2)
    relay(1)
    for d in range(3, line):
        relay(d)
    for s in range(last - 1):
        move(1, s)
        move(0, s)
        if s == 0:
            relay(2)
    early_count = len(pending)
    first(2)
    with jax.named_scope("weights_wait"):
        for keep in keeps:
            keep.wait()
        arrived("wy0", whole3(fs + 1 - 2 * y))
    for d in range(1, line):
        weights_done(d)

    def activations(x):
        pre = jnp.dot(x, gate_up[...], preferred_element_type=f32)
        g, u = pre[:, :layer], pre[:, layer:]
        s = jax.nn.sigmoid(g)
        return g, u, s, (g * s * u).astype(bf16)

    def early_block(place_of):
        here = block(place_of, rows, ROWS)
        g, u, s, h = activations(acts[0, here, :])
        grad_hidden = 0.5 * contract_cols(acts[1, here, :], down[...])
        hidden[here, :] = h
        grads[here, pl.ds(0, layer)] = (grad_hidden * u * s * (1.0 + g * (1.0 - s))).astype(bf16)
        grads[here, pl.ds(layer, layer)] = (grad_hidden * g * s).astype(bf16)

    with jax.named_scope("early_own"):
        early_block(z)
    for s in range(last):
        if s == last - 1:
            move(1, s)
            move(0, s)
        moved(1, s)
        moved(0, s)

        with jax.named_scope(f"early_{s}"):

            @pl.loop(0, 2)
            def _(d):
                to = z + (2 * d - 1) * (s + 1)
                pl.when((to >= 0) & (to < line))(lambda: early_block(to))

    order = list(range(1, line)) + [0]

    def weight_grads(owner):
        cols = block(owner, depth, LANES)
        gate_up_delta[block(owner, depth, ROWS), :] = contract_rows(
            acts[0, :, cols], grads[...]
        ).astype(bf16)
        down_delta[:, cols] = (0.5 * contract_rows(hidden[...], acts[1, :, cols])).astype(bf16)

    def deltas(owner):
        return [
            gate_up_delta.at[block(owner, depth, ROWS), :],
            down_delta.at[:, block(owner, depth, LANES)],
        ]

    lead = order[0]
    lead_z = place(lead)

    def lead_rows(who):
        return [
            gate_up_delta.at[block((lead_z * 2 + v) * 2 + who, deep, ROWS), :] for v in range(2)
        ]

    def lead_cols(who):
        return down_delta.at[block(who, tall, ROWS), block(lead_z, 2 * depth, LANES)]

    def y_send(k, a):
        src = deltas(place(k) * 2 + 1 - y)[1 - a]
        to = (y_gate_up if a else y_down).at[place(k)]
        go(copies(("gy", a, k), [src], [to], side))

    with jax.named_scope("wgrad_lead"):
        for v in range(2):
            weight_grads(lead_z * 2 + v)
    go(copies(("ax", 0), [lead_cols(1 - rep)], [a_down], twin))
    go(copies(("ax", 1), lead_rows(1 - rep), [a_gate_up.at[v] for v in range(2)], twin))
    for k in order[1:]:
        owner = place(k) * 2 + 1 - y
        with jax.named_scope(f"wgrad_{k}"):
            weight_grads(owner)
        if k == order[1]:
            y_send(k, 0)
            y_send(k, 1)

    @named
    def lead_x(a):
        if a:
            arrived(("ax", 1), [a_gate_up.at[v] for v in range(2)])
            for v, own in enumerate(lead_rows(rep)):
                add_strips(a_gate_up.at[v], own, a_gate_up.at[v])
            go(copies(("ay", 1), [a_gate_up.at[1 - y]], [x_gate_up.at[lead_z]], side))
            for k in order[2:3]:
                y_send(k, 1)
            for k in order[3:]:
                y_send(k, 0)
                y_send(k, 1)
        else:
            arrived(("ax", 0), [a_down])
            add_strips(a_down, lead_cols(rep), a_down)
            src = a_down.at[:, block(1 - y, depth, LANES)]
            go(copies(("ay", 0), [src], [x_down.at[lead_z]], side))
            for k in order[2:3]:
                y_send(k, 0)

    @named
    def to_mate(i):
        go(copies(("pm", i), [part.at[i, :, other]], [part_in.at[i]], mate))

    @named
    def from_mate(i):
        arrived(("pm", i), [part_in.at[i]])

        @pl.loop(0, line)
        def _(t):
            here = block(t, rows, ROWS)
            add_strips(sums.at[i, t], part.at[i, here, mine], part_in.at[i, here, :])

    def add_in(i, t, key, landed):
        arrived((key, i, t), [landed.at[i, t]])
        add_strips(sums.at[i, t], sums.at[i, t], landed.at[i, t])

    @named
    def chain(i, stage):
        for here in range(line):
            up = [("zu", t, here + last - t) for t in range(last, here, -1)]
            low = [("zd", t, last - here + t) for t in range(here)]
            for key, t, when in sorted(up + low, key=lambda v: v[2]):
                first_hop = here == (0 if key == "zu" else last)
                if stage != when:
                    continue
                landed, peer = (from_below, above) if key == "zu" else (from_above, below)
                if not first_hop:
                    on(z == here, functools.partial(add_in, i, t, key, landed))
                go(copies((key, i, t), [sums.at[i, t]], [landed.at[i, t]], peer), z == here)

    @named
    def finish(i):
        for t in range(line):
            if t > 0:
                on(z == t, functools.partial(add_in, i, t, "zu", from_below))
            if t < last:
                on(z == t, functools.partial(add_in, i, t, "zd", from_above))
        full[i, :, mine] = sums[i, z]
        go(copies(("fm", i), [full.at[i, :, mine]], [full.at[i, :, mine]], mate))

    @named
    def output(i):
        arrived(("fm", i), [full.at[i, :, other]])

        @pl.loop(0, rows // ROWS)
        def _(j):
            here = block(j, ROWS, ROWS)
            total = full[i, here, :].astype(f32)
            if i == 0:
                late = x_late[here, :].astype(f32)
                out_late[here, :] = (late + 0.5 * total).astype(bf16)
                return
            early = x_early[here, :].astype(f32)
            scale = scale_of(early)
            unit = early * scale
            inner = jnp.mean(total * unit, axis=-1, keepdims=True)
            kept = acts[1, pl.ds(pl.multiple_of(z * rows + j * ROWS, ROWS), ROWS), :].astype(f32)
            grad_in[here, :] = (kept + scale * (total - unit * inner)).astype(bf16)

    @named
    def y_step(k, a):
        t = place(k)
        landed, went = (y_gate_up, x_gate_up) if a else (y_down, x_down)
        arrived(("gy", a, k), [landed.at[t]])
        add_strips(landed.at[t], deltas(t * 2 + y)[1 - a], landed.at[t])
        src = landed.at[t, block(1 - rep, deep if a else tall, ROWS), :]
        go(copies(("gx", a, k), [src], [went.at[t]], twin))

    def landing(place_of, who, a):
        at_rows, at_cols = block(who, deep, ROWS), block(place_of, layer, LANES)
        if a:
            return [delta_gate.at[at_rows, at_cols], delta_up.at[at_rows, at_cols]]
        return [delta_down.at[block(place_of * 2 + who, tall, ROWS), :]]

    puts = []

    @named
    def x_step(k, a):
        t = place(k)
        landed, kept = (x_gate_up, y_gate_up) if a else (x_down, y_down)
        if k == lead:
            arrived(("ay", a), [landed.at[t]])
            own = a_gate_up.at[y] if a else a_down.at[:, block(y, depth, LANES)]
        else:
            arrived(("gx", a, k), [landed.at[t]])
            own = kept.at[t, block(rep, deep if a else tall, ROWS), :]
        add_strips(landed.at[t], own, landed.at[t])
        srcs = [landed.at[t]]
        if a:
            srcs = [landed.at[t, :, pl.ds(0, layer)], landed.at[t, :, pl.ds(layer, layer)]]
        to = landing(z, rep, a)
        if k:
            go(copies(("gz", a, k), srcs, to, {"fs": lax.rem(fs + 2 * k, n)}))
            return
        go(copies(("gt", a, 0), srcs, to, twin))
        for i, (s, d) in enumerate(zip(srcs, to)):
            put = pltpu.make_async_copy(s, d, local.at[a + i])
            put.start()
            puts.append(put)

    @named
    def z_step(k, a):
        refs = landing(origin(k), rep, a)
        arrived(("gz", a, k), refs)
        go(copies(("gt", a, k), refs, refs, twin))

    def columns(i, who):
        @pl.loop(0, half // wide)
        def _(j):
            cols = block(who * (half // wide) + j, wide, LANES)
            if i:
                at_rows = block(who * (half // wide) + j, wide, ROWS)
                product = contract_cols(grads[...], gate_up[at_rows, :])
            else:
                product = jnp.dot(hidden[...], down[:, cols], preferred_element_type=f32)
            part[i, :, cols] = product.astype(bf16)

    @named
    def partials(i):
        columns(i, 1 - tp)
        to_mate(i)
        columns(i, tp)

    @named
    def late_hidden():
        for s in range(last):
            moved(2, s)

        @pl.loop(0, line)
        def _(t):
            here = block(t, rows, ROWS)
            hidden[here, :] = activations(acts[2, here, :])[3]

    for s in range(last - 2):
        move(2, s)
    partials(1)
    with jax.named_scope("recycle"):
        drain(pending[:early_count])
        free.extend(group[0] for _, group in pending[:early_count])
        del pending[:early_count]

    @named
    def wgrad_own():
        for k in order[1:]:
            weight_grads(place(k) * 2 + y)

    plan = ["a0", "w", "y20", "m", "c10", "v", "a1", "y21", "h", "x20", "x10", "c11", "p", "x21"]
    plan += ["y30", "n", "c00", "x11", "z10", "z20", "c12", "x30", "y31", "y00", "c01", "x31"]
    plan += ["z21", "x00", "z11", "y01", "z30", "x01", "f1", "c02", "z31", "o1", "f0", "o0"]
    if line != 4:
        plan = ["w", "m", "v", "h", "p", "n", "a0", "a1"]
        plan += [f"c{i}{stage}" for i in (1, 0) for stage in range(last)]
        plan += [f"y{k}{a}" for k in order[1:] for a in (0, 1)]
        plan += [f"{step}{k}{a}" for k in order for step in "xz" for a in (0, 1) if k or step < "z"]
        plan += ["f1", "f0", "o1", "o0"]
    steps = {"y": y_step, "x": x_step, "z": z_step, "c": chain}
    single = {
        "a0": lambda: lead_x(0),
        "a1": lambda: lead_x(1),
        "w": wgrad_own,
        "m": lambda: from_mate(1),
        "n": lambda: from_mate(0),
        "h": late_hidden,
        "p": lambda: partials(0),
        "f1": lambda: finish(1),
        "f0": lambda: finish(0),
        "o1": lambda: output(1),
        "o0": lambda: output(0),
    }

    def late_moves():
        for s in range(max(last - 2, 0), last):
            move(2, s)

    single["v"] = late_moves
    for name in plan:
        if name in single:
            single[name]()
        else:
            steps[name[0]](int(name[1]), int(name[2:]))
    with jax.named_scope("last_in"):
        for a in range(2):
            for k in order:
                arrived(("gt", a, k), landing(origin(k), 1 - rep, a))

    with jax.named_scope("drain"):
        for put in puts:
            put.wait()
        assert len(names) <= recv.shape[0] and len(made) <= send.shape[0]
        drain(pending)


def fast_shards(n, x_early, x_late, grad_out, w_gate, w_up, w_down, gate_sum, up_sum, down_sum):
    bf16 = jnp.bfloat16
    shape = jax.ShapeDtypeStruct
    line = n // 2
    rows, width = x_early.shape
    hidden_here, depth = w_down.shape
    layer = hidden_here // line
    tokens, half = line * rows, width // 2
    dma, vmem = pltpu.SemaphoreType.DMA, pl.BlockSpec(memory_space=pltpu.VMEM)
    out_late, grad_in, delta_gate, delta_up, delta_down = pl.pallas_call(
        functools.partial(step_kernel, n),
        out_shape=[
            shape((rows, width), bf16),
            shape((rows, width), bf16),
            shape((depth, hidden_here), bf16),
            shape((depth, hidden_here), bf16),
            shape((hidden_here, depth), bf16),
        ],
        in_specs=[pl.BlockSpec(memory_space=pltpu.HBM)] * 6,
        out_specs=[vmem, vmem, ANY, ANY, ANY],
        scratch_shapes=[
            pltpu.VMEM((3, tokens, width), bf16),
            pltpu.VMEM((width, 2 * layer), bf16),
            pltpu.VMEM((layer, width), bf16),
            pltpu.VMEM((tokens, layer), bf16),
            pltpu.VMEM((tokens, 2 * layer), bf16),
            pltpu.VMEM((2, tokens, width), bf16),
            pltpu.VMEM((2, tokens, half), bf16),
            pltpu.VMEM((2, line, rows, half), bf16),
            pltpu.VMEM((2, line, rows, half), bf16),
            pltpu.VMEM((2, line, rows, half), bf16),
            pltpu.VMEM((width, 2 * layer), bf16),
            pltpu.VMEM((layer, width), bf16),
            pltpu.VMEM((line, depth, 2 * layer), bf16),
            pltpu.VMEM((line, layer, depth), bf16),
            pltpu.VMEM((line, depth // 2, 2 * layer), bf16),
            pltpu.VMEM((line, layer // 2, depth), bf16),
            pltpu.VMEM((2, depth // 2, 2 * layer), bf16),
            pltpu.VMEM((layer // 2, 2 * depth), bf16),
            pltpu.VMEM((2, rows, width), bf16),
            pltpu.VMEM((rows, width), bf16),
            pltpu.VMEM((rows, width), bf16),
            dma((22 * line - 14,)),
            dma((32 * line - 21,)),
            dma((6,)),
        ],
        compiler_params=pltpu.CompilerParams(
            collective_id=0, has_side_effects=True, vmem_limit_bytes=60 * 2**20
        ),
    )(x_early, x_late, grad_out, w_gate, w_up, w_down)
    out_late, grad_in, new_gate, new_up, new_down = settle(
        out_late, grad_in, gate_sum, up_sum, down_sum, delta_gate, delta_up, delta_down
    )
    return out_late, grad_in, new_gate, new_up, new_down


PARTS = 2


def settle_kernel(*refs):
    ins, outs, held, sem = refs[:8], refs[8:13], refs[13:21], refs[21]
    loads = [pltpu.make_async_copy(ins[i], held[i], sem.at[i]) for i in range(8)]
    for i in (2, 5, 3, 6, 4, 7, 0, 1):
        loads[i].start()
    stores = []

    def store(src, dst):
        copy = pltpu.make_async_copy(src, dst, sem.at[8 + len(stores)])
        copy.start()
        stores.append(copy)

    for i in range(2, 5):
        loads[i].wait()
        loads[i + 3].wait()
        total, delta = held[i], held[i + 3]
        size = total.shape[0] // PARTS
        for p in range(PARTS):

            @pl.loop(0, size // ROWS)
            def _(j):
                at = pl.ds(pl.multiple_of(p * size + j * ROWS, ROWS), ROWS)
                total[at, :] = total[at, :] + delta[at, :].astype(jnp.float32)

            at = pl.ds(p * size, size)
            store(total.at[at, :], outs[i].at[at, :])
        if i == 2:
            for k in range(2):
                loads[k].wait()
                store(held[k], outs[k])
    for copy in stores:
        copy.wait()


def settle(*args):
    outs = [jax.ShapeDtypeStruct(v.shape, v.dtype) for v in args[:5]]
    size = sum(v.size for v in args[2:5])
    return pl.pallas_call(
        settle_kernel,
        out_shape=outs,
        in_specs=[ANY] * 8,
        out_specs=[ANY] * 5,
        scratch_shapes=[pltpu.VMEM(v.shape, v.dtype) for v in args]
        + [pltpu.SemaphoreType.DMA((10 + 3 * PARTS,))],
        cost_estimate=pl.CostEstimate(flops=size, bytes_accessed=10 * size, transcendentals=0),
    )(*args)


def shards(x_early, x_late, grad_out, w_gate, w_up, w_down, gate_sum, up_sum, down_sum):
    gate_full, up_full, down_full = (
        lax.all_gather(w_gate, "fs", axis=0, tiled=True),
        lax.all_gather(w_up, "fs", axis=0, tiled=True),
        lax.all_gather(w_down, "fs", axis=1, tiled=True),
    )
    batch_rows = x_early.shape[0]
    stacked = jnp.concatenate([x_early, x_late], axis=0).astype(jnp.float32)
    row_scale = lax.rsqrt(jnp.mean(stacked * stacked, axis=-1, keepdims=True) + epsilon)
    normed = (stacked * row_scale).astype(jnp.bfloat16)
    gate_pre = jnp.dot(normed, gate_full, preferred_element_type=jnp.float32)
    up_pre = jnp.dot(normed, up_full, preferred_element_type=jnp.float32)
    gate_sig = jax.nn.sigmoid(gate_pre)
    hidden = (gate_pre * gate_sig * up_pre).astype(jnp.bfloat16)
    late_part = jnp.dot(hidden[batch_rows:], down_full, preferred_element_type=jnp.float32).astype(
        jnp.bfloat16
    )
    branch = lax.psum(late_part, "tp").astype(jnp.float32)
    out_late = (stacked[batch_rows:] + 0.5 * branch).astype(jnp.bfloat16)
    early_gate = gate_pre[:batch_rows]
    early_upper = up_pre[:batch_rows]
    early_sig = gate_sig[:batch_rows]
    early_hidden = hidden[:batch_rows]
    early_normed = normed[:batch_rows]
    early_scale = row_scale[:batch_rows]
    grad_hidden = 0.5 * contract_cols(grad_out, down_full)
    grad_gate_in = (
        grad_hidden * early_upper * early_sig * (1.0 + early_gate * (1.0 - early_sig))
    ).astype(jnp.bfloat16)
    grad_up_in = (grad_hidden * early_gate * early_sig).astype(jnp.bfloat16)
    normed_part = contract_cols(grad_gate_in, gate_full) + contract_cols(grad_up_in, up_full)
    grad_normed = lax.psum(normed_part.astype(jnp.bfloat16), "tp").astype(jnp.float32)
    unit_rows = stacked[:batch_rows] * early_scale
    inner = jnp.mean(grad_normed * unit_rows, axis=-1, keepdims=True)
    grad_in = (
        grad_out.astype(jnp.float32) + early_scale * (grad_normed - unit_rows * inner)
    ).astype(jnp.bfloat16)
    normed_cols, out_cols = (
        lax.all_to_all(early_normed, "fs", split_axis=1, concat_axis=0, tiled=True),
        lax.all_to_all(grad_out, "fs", split_axis=1, concat_axis=0, tiled=True),
    )
    gate_delta = contract_rows(normed_cols, lax.all_gather(grad_gate_in, "fs", axis=0, tiled=True))
    up_delta = contract_rows(normed_cols, lax.all_gather(grad_up_in, "fs", axis=0, tiled=True))
    down_half = contract_rows(lax.all_gather(early_hidden, "fs", axis=0, tiled=True), out_cols)
    down_delta = 0.5 * down_half
    gate_delta, up_delta, down_delta = (
        lax.psum(gate_delta.astype(jnp.bfloat16), "rep").astype(jnp.float32),
        lax.psum(up_delta.astype(jnp.bfloat16), "rep").astype(jnp.float32),
        lax.psum(down_delta.astype(jnp.bfloat16), "rep").astype(jnp.float32),
    )
    return (out_late, grad_in, gate_sum + gate_delta, up_sum + up_delta, down_sum + down_delta)


def shards_for(mesh):
    n, reps, cores = mesh.shape["fs"], mesh.shape["rep"], mesh.shape["tp"]

    def run(*args):
        rows, width = args[0].shape
        hidden_here, depth = args[5].shape
        line = max(n // 2, 1)
        layer = hidden_here // line
        fits = (
            reps == 2
            and cores == 2
            and n % 2 == 0
            and n >= 4
            and rows % ROWS == 0
            and width % (2 * LANES) == 0
            and depth % (2 * LANES) == 0
            and hidden_here % line == 0
            and layer % LANES == 0
            and layer % (2 * ROWS) == 0
            and 2 * (10 * line * rows * width + 10 * width * layer) < 44 * 2**20
        )
        return fast_shards(n, *args) if fits else shards(*args)

    return run


def solution(mesh):
    placed = (
        P(("rep", "fs"), None),
        P(("rep", "fs"), None),
        P(("rep", "fs"), None),
        P("fs", "tp"),
        P("fs", "tp"),
        P("tp", "fs"),
        P("fs", "tp"),
        P("fs", "tp"),
        P("tp", "fs"),
    )
    return jax.shard_map(
        shards_for(mesh),
        mesh=mesh,
        in_specs=placed,
        out_specs=(
            P(("rep", "fs"), None),
            P(("rep", "fs"), None),
            P("fs", "tp"),
            P("fs", "tp"),
            P("tp", "fs"),
        ),
        check_vma=False,
    )
```
